32 devices in a mesh: rep: 4 (over z), fs: 4 (over y, x), tp: 2 (over core).
Axes of the slice: x: 2, y: 2, z: 4, core: 2. Of those that a mesh axis runs over, the one named last changes fastest.
Arguments:
- hidden_in: bfloat16 [2048, 2048], P('rep'), may hold values from -6 to 6
- cotangent: bfloat16 [2048, 2048], P('rep'), may hold values from -3 to 3
- w_up: bfloat16 [2048, 8192], P('rep', ('fs', 'tp')), may hold values from -0.125 to 0.125
- w_down: bfloat16 [8192, 2048], P(('fs', 'tp'), 'rep'), may hold values from -0.0625 to 0.0625
Outputs:
- input_grad: bfloat16 [2048, 2048], P('rep')
- up_grad: float32 [2048, 8192], P('rep', ('fs', 'tp'))
- down_grad: float32 [8192, 2048], P(('fs', 'tp'), 'rep')
The draws below stay inside these ranges and needn't reach their ends.
All inputs are finite; a program needn't handle non-finite values.
Results may differ from the reference program's by a relative error of at most 0.017.
Values may be sent and summed in bfloat16 or wider, within the bound.
A program may use at most 64 MiB of HBM per device.

```python
import jax
import jax.numpy as jnp
from jax import lax

D = 2048
FF = 8192
TOKENS = 2048
N_FS = 4
N_TP = 2


def strengthened(drawn, key, source, target, parts, factor):
    def block_of(dim):
        return (jnp.arange(drawn.shape[dim]) // (drawn.shape[dim] // parts)).reshape((-1,) + (1,) * (drawn.ndim - 1 - dim))

    near = jax.random.permutation(key, parts)[block_of(target)]
    other_side = (block_of(target) + parts // 2) % parts
    return jnp.where((block_of(source) == near) | (block_of(source) == other_side), factor * drawn, drawn)


def level_of(stream_key, dims, pieces, low, largest):
    level = 1.0
    for position, parts in pieces:
        steps = jax.random.uniform(jax.random.fold_in(jax.random.fold_in(stream_key, 6), position), (parts,), jnp.float32, low / len(pieces), largest / len(pieces))
        level = level * jnp.repeat(jnp.exp(steps), dims[position] // parts).reshape((-1,) + (1,) * (len(dims) - 1 - position))
    return level


def noise(key, extent, width, reach, pieces=(), dtype=jnp.bfloat16):
    drawn = width * jax.random.normal(key, extent, jnp.float32)
    if pieces:
        drawn = drawn * level_of(key, extent, pieces, -0.22, 0.18)
    return jnp.clip(drawn, -reach, reach).astype(dtype)


def heavy_noise(key, shape, width, bound, split, heavy, kind=jnp.bfloat16):
    values = width * jax.random.normal(key, shape, jnp.float32)
    if split:
        values = values * level_of(key, shape, split, -0.22, 0.18)
    return jnp.clip(strengthened(values, jax.random.fold_in(key, 3), *heavy), -bound, bound).astype(kind)


def setup_inputs(seed: int = 0) -> dict:
    splits = jax.random.split(jax.random.key(seed), 5)
    hidden_in = heavy_noise(splits[0], (TOKENS, D), 1.0, 6.0, ((0, 4),), (0, 1, 4, 2.0))
    cotangent = heavy_noise(splits[1], (TOKENS, D), 0.5, 3.0, ((0, 4),), (0, 1, 4, 2.0))
    w_up = noise(splits[2], (D, FF), D ** -0.5, 0.125, ((0, 4), (1, 8)))
    w_down = noise(splits[3], (FF, D), FF ** -0.5, 0.0625, ((0, 8), (1, 4)))
    return dict(hidden_in=hidden_in, cotangent=cotangent, w_up=w_up, w_down=w_down)


def contract_last(left, right):
    return lax.dot_general(left, right, (((1,), (1,)), ((), ())), preferred_element_type=jnp.float32)


def contract_first(left, right):
    return lax.dot_general(left, right, (((0,), (0,)), ((), ())), preferred_element_type=jnp.float32)


def reference(hidden_in, cotangent, w_up, w_down):
    blocks = N_FS * N_TP
    block_cols = FF // blocks
    up_blocks = jnp.transpose(w_up.reshape(D, blocks, block_cols), (1, 0, 2))
    down_blocks = w_down.reshape(blocks, block_cols, D)

    def one_block(summed, weights):
        up_part, down_part = weights
        preact = jnp.dot(hidden_in, up_part, preferred_element_type=jnp.float32)
        back_grad = contract_last(cotangent, down_part)
        active = jnp.maximum(preact, 0.0)
        hidden = (active * active).astype(jnp.bfloat16)
        slopes = (2.0 * active * back_grad).astype(jnp.bfloat16)
        part_sum = lax.optimization_barrier(contract_last(slopes, up_part).astype(jnp.bfloat16))
        summed = summed + part_sum.astype(jnp.float32)
        grad_upper = contract_first(hidden_in, slopes)
        grad_lower = contract_first(hidden, cotangent)
        return summed, (grad_upper, grad_lower)

    summed, (grads_upper, grads_lower) = lax.scan(
        one_block, jnp.zeros((TOKENS, D), jnp.float32), (up_blocks, down_blocks))
    input_grad = summed.astype(jnp.bfloat16)
    up_grad = jnp.transpose(grads_upper, (1, 0, 2)).reshape(D, FF)
    down_grad = grads_lower.reshape(FF, D)
    return (input_grad, up_grad, down_grad)
```

```python
import functools

import jax
import jax.numpy as jnp
from jax import lax
from jax.experimental import pallas as pl
from jax.experimental.pallas import tpu as pltpu
from jax.sharding import PartitionSpec as P

MESH = pl.DeviceIdType.MESH
BF16, F32 = jnp.bfloat16, jnp.float32


def contract_last(left, right):
    return lax.dot_general(left, right, (((1,), (1,)), ((), ())), preferred_element_type=F32)


def contract_first(left, right):
    return lax.dot_general(left, right, (((0,), (0,)), ((), ())), preferred_element_type=F32)


def plain(hidden_in, cotangent, w_up, w_down):
    up_full = lax.all_gather(w_up, "rep", axis=0, tiled=True)
    back_grad = contract_last(cotangent, lax.all_gather(w_down, "rep", axis=1, tiled=True))
    preact = jnp.dot(hidden_in, up_full, preferred_element_type=F32)
    active = jnp.maximum(preact, 0.0)
    hidden = (active * active).astype(BF16)
    slopes = (2.0 * active * back_grad).astype(BF16)
    grad_upper = lax.psum_scatter(
        contract_first(hidden_in, slopes).astype(BF16), "rep", scatter_dimension=0, tiled=True
    ).astype(F32)
    lower_rows = lax.psum_scatter(
        contract_first(cotangent, hidden).astype(BF16), "rep", scatter_dimension=0, tiled=True
    ).astype(F32)
    partial_sum = contract_last(slopes, up_full).astype(BF16)
    input_grad = lax.psum(partial_sum, ("fs", "tp")).astype(F32).astype(BF16)
    return (input_grad, grad_upper, lower_rows.T)


SC = jax.named_scope

def kernel(
    R, x_ref, g_ref, wu_in, wd_in,
    ig_ref, ru_ref, rd_ref,
    tok, wu, wd, act, slopes, s_t, h_t, part, r0, r1, r2, r3, ug, dg,
    send_sems, recv_sems, local_sems,
):
    z, f, c = lax.axis_index("rep"), lax.axis_index("fs"), lax.axis_index("tp")
    tl, D = x_ref.shape
    dl, fl = wu_in.shape
    h = fl // R
    pr = tl // 8
    half = 4 * pr
    steps = 2 * (R - 1)
    xx, yy = lax.rem(f, 2), lax.div(f, 2)
    fx, fy = yy * 2 + (1 - xx), (1 - yy) * 2 + xx
    f1 = fx * (1 - c) + fy * c
    f2 = fy * (1 - c) + fx * c
    f3 = 3 - f

    edge = jnp.minimum(z, R - 1 - z)
    far = jnp.where(z < R - 1 - z, 1, -1)
    inner = edge > 0
    outer = edge == 0

    def plane_at(slot):
        both = z + (slot // 2 + 1) * (2 * (slot % 2) - 1) * far
        return jnp.where(slot < 2 * edge, both, z + far * (slot + 1 - edge))

    near_first = [plane_at(slot) for slot in range(R - 1)]
    far_first = near_first[::-1]
    blocks = far_first + [z]

    def beyond(p):
        return jnp.logical_or(jnp.logical_and(p < z, z < R - 1), jnp.logical_and(p > z, z > 0))

    def past(p):
        return jnp.where(p < z, z + 1, z - 1)

    def toward(p):
        return jnp.where(p > z, z + 1, z - 1)

    send_names, recv_names = {}, {}

    def named(names, key, count):
        if key not in names:
            names[key] = sum(n for _, n in names.values()), count
        return names[key][0]

    def dev(zz=None, ff=None, cc=None):
        return {"rep": z if zz is None else zz, "fs": f if ff is None else ff, "tp": c if cc is None else cc}

    def remote(src, dst, device, group, key, index=0, count=1):
        return pltpu.make_async_remote_copy(
            src_ref=src, dst_ref=dst, send_sem=send_sems.at[named(send_names, group, 1)],
            recv_sem=recv_sems.at[named(recv_names, key, count) + index],
            device_id=device, device_id_type=MESH)

    def send(*args, **kw):
        remote(*args, **kw).start()

    def arrived(dst, key, index=0, count=1):
        pltpu.make_async_remote_copy(
            src_ref=dst, dst_ref=dst, send_sem=send_sems.at[0],
            recv_sem=recv_sems.at[named(recv_names, key, count) + index],
            device_id=dev(cc=1 - c), device_id_type=MESH).wait_recv()

    def sent(src, group):
        pltpu.make_async_remote_copy(
            src_ref=src, dst_ref=src, send_sem=send_sems.at[named(send_names, group, 1)],
            recv_sem=recv_sems.at[0], device_id=dev(cc=1 - c), device_id_type=MESH).wait_send()

    def rows(zz, ff, cc):
        return pl.ds(pl.multiple_of(zz * tl + (cc * 4 + ff) * pr, pr), pr)

    def core_rows(zz, cc):
        return pl.ds(pl.multiple_of(zz * tl + cc * half, half), half)

    def piece_rows(ff, cc):
        return pl.ds(pl.multiple_of((cc * 4 + ff) * pr, pr), pr)

    def up_cols(zz):
        return pl.ds(pl.multiple_of(zz * h, h), h)

    def d_block(zz):
        return pl.ds(pl.multiple_of(zz * dl, dl), dl)

    with SC("barrier"):
        barrier = pltpu.get_barrier_semaphore()
        near = [dev(zz=lax.rem(z + d, R)) for d in range(1, R)] + [dev(ff=fx), dev(ff=fy), dev(cc=1 - c)]
        for device in near:
            pl.semaphore_signal(barrier, inc=1, device_id=device, device_id_type=MESH)
        pl.semaphore_wait(barrier, len(near))

    TOK = dict(key="tok", count=2 * R)
    sources = (x_ref, g_ref)
    own_sends = []
    for a in (0, 1):
        for side, (to, there) in enumerate(((z + 1, z < R - 1), (z - 1, z > 0))):
            copy = remote(sources[a].at[piece_rows(f, c), :], tok.at[a, rows(z, f, c), :],
                          dev(zz=to), ("own", a, side), index=a * R + z, **TOK)
            pl.when(there)(copy.start)
            own_sends.append((copy, there))

    def send_up(p):
        send(wu_in.at[:, up_cols(p)], wu.at[d_block(z), :], dev(zz=p), "wu", "wu")

    def send_down(p):
        send(wd_in.at[up_cols(p), :], wd.at[:, d_block(z)], dev(zz=p), "wd", "wd")

    @pl.when(outer)
    def _():
        for p in near_first[:1] + far_first[:-1]:
            send_up(p)
        for p in far_first:
            send_down(p)

    own_rows = pl.ds(pl.multiple_of(z * tl, tl), tl)
    local = [
        pltpu.make_async_copy(x_ref, tok.at[0, own_rows, :], local_sems.at[0]),
        pltpu.make_async_copy(g_ref, tok.at[1, own_rows, :], local_sems.at[1]),
        pltpu.make_async_copy(wu_in.at[:, up_cols(z)], wu.at[d_block(z), :], local_sems.at[2]),
        pltpu.make_async_copy(wd_in.at[up_cols(z), :], wd.at[:, d_block(z)], local_sems.at[3]),
    ]
    for copy in local:
        copy.start()

    outer_order = [(a, slot) for slot in range(R - 1) for a in (0, 1)]
    inner_order = [(a, slot) for pair in range(0, R - 1, 2) for a in (0, 1)
                   for slot in range(pair, min(pair + 2, R - 1))]
    order = []
    for (ai, si), (ao, so) in zip(inner_order, outer_order):
        a = ai if ai == ao else jnp.where(inner, ai, ao)
        p = near_first[si] if si == so else jnp.where(inner, near_first[si], near_first[so])
        order.append((a, p))

    def spread(at, tag):
        group = tag + ("sent",)

        def first():
            mine = at(f, c)
            send(mine, mine, dev(ff=f1), group, tag + (1,))
            send(mine, mine, dev(ff=f2), group, tag + (2,))
            send(mine, mine, dev(cc=1 - c), group, tag + (4,))

        def second():
            p1, p2 = at(f1, c), at(f2, c)
            arrived(p1, tag + (1,))
            send(p1, p1, dev(ff=f2), group, tag + (3,))
            send(p1, p1, dev(cc=1 - c), group, tag + (4,))
            arrived(p2, tag + (2,))
            send(p2, p2, dev(cc=1 - c), group, tag + (4,))

        def third():
            p3 = at(f3, c)
            arrived(p3, tag + (3,))
            send(p3, p3, dev(cc=1 - c), group, tag + (4,))

        return first, second, third

    spreads = [
        spread(lambda ff, cc, a=a, p=p: tok.at[a, rows(p, ff, cc), :], ("tok", i))
        for i, (a, p) in enumerate(order)
    ]

    def forward(i):
        a, p = order[i]
        mine = tok.at[a, rows(p, f, c), :]
        return remote(mine, mine, dev(zz=past(p)), ("fwd", i), index=a * R + p, **TOK)

    def take(i):
        a, p = order[i]
        arrived(tok.at[a, rows(p, f, c), :], index=a * R + p, **TOK)
        pl.when(beyond(p))(forward(i).start)

    def first(i):
        with SC(f"first{i}"): spreads[i][0]()

    def second(i):
        with SC(f"second{i}"): spreads[i][1]()

    def third(i):
        with SC(f"third{i}"): spreads[i][2]()

    def last(i):
        a, p = order[i]
        with SC(f"last{i}"): arrived(tok.at[a, core_rows(p, 1 - c), :], ("tok", i, 4))

    def take_in(*which):
        @pl.when(inner)
        def _():
            for i in which:
                if i < steps:
                    with SC(f"takeI{i}"): take(i)

    def take_out(*which):
        @pl.when(outer)
        def _():
            for i in which:
                if i < steps:
                    with SC(f"takeO{i}"): take(i)

    with SC("take0"): take(0)
    first(0)
    with SC("take1"): take(1)
    first(1)
    take_in(2, 3)

    inward = [p for p in far_first]

    @pl.when(inner)
    def _():
        for p in far_first:
            pl.when((p - z) * far > 0)(functools.partial(send_up, p))

    second(0)
    take_out(2)
    first(2)
    second(1)
    third(0)
    take_in(4)
    take_out(3)
    first(3)
    second(2)
    third(1)
    take_in(5)

    @pl.when(inner)
    def _():
        for p in far_first:
            pl.when((p - z) * far < 0)(functools.partial(send_up, p))
        for p in far_first:
            send_down(p)

    second(3)
    third(2)
    take_out(4)
    first(4)
    second(4)
    third(3)
    take_out(5)
    first(5)
    second(5)
    third(4)

    step = min(tl, 256)

    def up_block(p):
        @pl.loop(0, tl // step)
        def _(i):
            at = pl.ds(pl.multiple_of(p * tl + i * step, step), step)
            active = jnp.maximum(jnp.dot(tok[0, at, :], wu[...], preferred_element_type=F32), 0.0)
            act[at, :] = active
            h_t[:, at] = jnp.transpose(active * active).astype(BF16)

    for copy in local:
        copy.wait()
    others = (R - 1) * dl
    with SC("wuwait"): arrived(wu.at[pl.ds(0, others), :], "wu")
    with SC("upz"): up_block(z)
    for i in range(4):
        last(i)
    with SC("up0"): up_block(near_first[0])
    with SC("up1"): up_block(near_first[1])
    third(5)
    last(4)
    with SC("up2"): up_block(near_first[2])
    last(5)

    def down_part(p):
        at = d_block(p)
        dg[:, at] = jnp.dot(h_t[...], tok[1, :, at], preferred_element_type=F32).astype(BF16)

    for p in far_first:
        with SC("downpart"): down_part(p)
        send(dg.at[:, d_block(p)], rd_ref.at[up_cols(z), :], dev(zz=p), "rd", "rd")
    with SC("downpartz"):
        down_part(z)
        rd_ref[up_cols(z), :] = dg[:, d_block(z)]

    with SC("wdwait"): arrived(wd.at[:, pl.ds(0, others)], "wd")

    def r0_rows(j, ff=None):
        if ff is None:
            return pl.ds(j * half, half)
        return pl.ds(pl.multiple_of(j * half + ff * pr, pr), pr)

    def added(*terms):
        total = terms[0].astype(F32)
        for term in terms[1:]:
            total = total + term.astype(F32)
        return total.astype(BF16)

    def core_sum(j):
        p = blocks[j]
        arrived(r0.at[r0_rows(j), :], ("r0", j))
        for k, ff in ((1, f3), (0, f1), (None, f2), (None, f)):
            at = rows(p, ff, c)
            part[at, :] = added(part[at, :], r0[r0_rows(j, ff), :])
            if k is not None:
                send(part.at[at, :], r1.at[j, k], dev(ff=f1), "r1", ("r1", j, k))

    def part_rows(at):
        value = 2.0 * act[at, :] * contract_last(tok[1, at, :], wd[...])
        slopes[at, :] = value.astype(BF16)
        part[at, :] = contract_last(slopes[at, :], wu[...]).astype(BF16)

    for j, p in enumerate(blocks):
        theirs = core_rows(p, 1 - c)
        with SC(f"slopesA{j}"): part_rows(theirs)
        send(part.at[theirs, :], r0.at[r0_rows(j), :], dev(cc=1 - c), "r0", ("r0", j))
        with SC(f"slopesB{j}"): part_rows(core_rows(p, c))
        if j:
            with SC(f"core{j-1}"): core_sum(j - 1)
    with SC(f"core{R-1}"): core_sum(R - 1)

    with SC("s_t"):
        @pl.loop(0, R * tl // step)
        def _(i):
            at = pl.ds(pl.multiple_of(i * step, step), step)
            s_t[:, at] = jnp.transpose(slopes[at, :].astype(F32)).astype(BF16)

    def first_sum(j):
        for k, ff in ((1, f2), (0, f)):
            at = rows(blocks[j], ff, c)
            arrived(r1.at[j, k], ("r1", j, k))
            part[at, :] = added(part[at, :], r1[j, k])
            if k:
                send(part.at[at, :], r2.at[j], dev(ff=f2), "r2", ("r2", j))

    def second_sum(j):
        at = rows(blocks[j], f, c)
        arrived(r2.at[j], ("r2", j))
        part[at, :] = added(part[at, :], r2[j])

    R3 = dict(key="r3", count=2 * R)

    def line_sum(j):
        p = blocks[j]
        at = rows(p, f, c)
        side = jnp.where(p > z, 0, 1)

        @pl.when(beyond(p))
        def _():
            arrived(r3.at[p, side], index=p * 2 + side, **R3)
            part[at, :] = added(part[at, :], r3[p, side])

        send(part.at[at, :], r3.at[p, side], dev(zz=toward(p)), "r3", index=p * 2 + side, **R3)

    def own_sum():
        at = rows(z, f, c)
        for side, there in ((0, z > 0), (1, z < R - 1)):
            @pl.when(there)
            def _(side=side):
                arrived(r3.at[z, side], index=z * 2 + side, **R3)
                part[at, :] = added(part[at, :], r3[z, side])
        ig_ref[piece_rows(f, c), :] = part[at, :]

    def up_part(p):
        at = d_block(p)
        ug[at, :] = jnp.transpose(jnp.dot(s_t[...], tok[0, :, at], preferred_element_type=F32)).astype(BF16)

    def send_up_part(p):
        with SC("uppart"): up_part(p)
        send(ug.at[d_block(p), :], ru_ref.at[:, up_cols(z)], dev(zz=p), "ru", "ru")

    chain = (first_sum, second_sum, line_sum)
    for i in range(R + 2):
        if i < R - 1:
            send_up_part(far_first[i])
        if i == R - 1:
            with SC("uppartz"):
                up_part(z)
                ru_ref[:, up_cols(z)] = ug[d_block(z), :]
        for back in (2, 1, 0):
            j = i - back
            if 0 <= j < R and not (back == 2 and j == R - 1):
                with SC(f"chain{back}.{j}"): chain[back](j)

    with SC("own"): own_sum()

    def part_of(n):
        rows_of = lambda ff, cc: pl.ds(pl.multiple_of((cc * 4 + ff) * pr + n * (pr // 2), pr // 2), pr // 2)
        return spread(lambda ff, cc: ig_ref.at[rows_of(ff, cc), :], ("ig", n))

    for k, pair in enumerate(zip(part_of(0), part_of(1))):
        for n, stage in enumerate(pair):
            with SC(f"ig{k}.{n}"): stage()
    with SC("iglast"):
        for n in (0, 1):
            arrived(ig_ref.at[pl.ds(0, half // 2), :], ("ig", n, 4))

    with SC("rdwait"): arrived(rd_ref.at[pl.ds(0, (R - 1) * h), :], "rd")
    with SC("ruwait"): arrived(ru_ref.at[:, pl.ds(0, (R - 1) * h)], "ru")

    with SC("sendwait"):
        for copy, there in own_sends:
            pl.when(there)(copy.wait_send)
        for i, (a, p) in enumerate(order):
            pl.when(beyond(p))(forward(i).wait_send)
            sent(part.at[pl.ds(0, 7 * pr), :], ("tok", i, "sent"))
        for n in (0, 1):
            sent(part.at[pl.ds(0, 7 * pr // 2), :], ("ig", n, "sent"))
        sent(wu.at[pl.ds(0, others), :], "wu")
        sent(wd.at[:, pl.ds(0, others)], "wd")
        sent(dg.at[:, pl.ds(0, others)], "rd")
        sent(ug.at[pl.ds(0, others), :], "ru")
        sent(r0, "r0")
        sent(r1, "r1")
        sent(r2, "r2")
        sent(part.at[pl.ds(0, (R - 1) * pr), :], "r3")
    for names, sems in ((send_names, send_sems), (recv_names, recv_sems)):
        assert sum(n for _, n in names.values()) == sems.shape[0], (names, sems.shape)


def in_planes(R, hidden_in, cotangent, w_up, w_down):
    tl, D = hidden_in.shape
    dl, fl = w_up.shape
    T, h, pr = tl * R, fl // R, tl // 8
    send_sems, recv_sems = 4 * R + 10, 16 * R + 4
    vmem = pl.BlockSpec(memory_space=pltpu.VMEM)
    input_grad, up, down = pl.pallas_call(
        functools.partial(kernel, R),
        out_shape=(
            pltpu.VMEM((tl, D), BF16),
            pltpu.VMEM((dl, fl), BF16),
            pltpu.VMEM((fl, dl), BF16),
        ),
        in_specs=[pl.BlockSpec(memory_space=pl.ANY)] * 4,
        out_specs=(vmem, vmem, vmem),
        scratch_shapes=[
            pltpu.VMEM((2, T, D), BF16),
            pltpu.VMEM((D, h), BF16),
            pltpu.VMEM((h, D), BF16),
            pltpu.VMEM((T, h), F32),
            pltpu.VMEM((T, h), BF16),
            pltpu.VMEM((h, T), BF16),
            pltpu.VMEM((h, T), BF16),
            pltpu.VMEM((T, D), BF16),
            pltpu.VMEM((R * 4 * pr, D), BF16),
            pltpu.VMEM((R, 2, pr, D), BF16),
            pltpu.VMEM((R, pr, D), BF16),
            pltpu.VMEM((R, 2, pr, D), BF16),
            pltpu.VMEM((D, h), BF16),
            pltpu.VMEM((h, D), BF16),
            pltpu.SemaphoreType.DMA((send_sems,)),
            pltpu.SemaphoreType.DMA((recv_sems,)),
            pltpu.SemaphoreType.DMA((4,)),
        ],
        compiler_params=pltpu.CompilerParams(
            collective_id=0, has_side_effects=True, vmem_limit_bytes=58 * 1024 * 1024
        ),
    )(hidden_in, cotangent, w_up, w_down)
    return input_grad, up.astype(F32), down.astype(F32)


def solution(mesh):
    R, F, C = (mesh.shape[name] for name in ("rep", "fs", "tp"))
    body = functools.partial(in_planes, R) if (F, C) == (4, 2) else plain
    return jax.shard_map(
        body,
        mesh=mesh,
        in_specs=(P("rep", None), P("rep", None), P("rep", ("fs", "tp")), P(("fs", "tp"), "rep")),
        out_specs=(P("rep", None), P("rep", ("fs", "tp")), P(("fs", "tp"), "rep")),
        check_vma=False,
    )
```

```python
import functools

import jax
import jax.numpy as jnp
from jax import lax
from jax.experimental import pallas as pl
from jax.experimental.pallas import tpu as pltpu
from jax.sharding import PartitionSpec as P

MESH = pl.DeviceIdType.MESH
BF16, F32 = jnp.bfloat16, jnp.float32


def contract_last(left, right):
    return lax.dot_general(left, right, (((1,), (1,)), ((), ())), preferred_element_type=F32)


def contract_first(left, right):
    return lax.dot_general(left, right, (((0,), (0,)), ((), ())), preferred_element_type=F32)


def plain(hidden_in, cotangent, w_up, w_down):
    up_full = lax.all_gather(w_up, "rep", axis=0, tiled=True)
    back_grad = contract_last(cotangent, lax.all_gather(w_down, "rep", axis=1, tiled=True))
    preact = jnp.dot(hidden_in, up_full, preferred_element_type=F32)
    active = jnp.maximum(preact, 0.0)
    hidden = (active * active).astype(BF16)
    slopes = (2.0 * active * back_grad).astype(BF16)
    grad_upper = lax.psum_scatter(
        contract_first(hidden_in, slopes).astype(BF16), "rep", scatter_dimension=0, tiled=True
    ).astype(F32)
    lower_rows = lax.psum_scatter(
        contract_first(cotangent, hidden).astype(BF16), "rep", scatter_dimension=0, tiled=True
    ).astype(F32)
    partial_sum = contract_last(slopes, up_full).astype(BF16)
    input_grad = lax.psum(partial_sum, ("fs", "tp")).astype(F32).astype(BF16)
    return (input_grad, grad_upper, lower_rows.T)


SC = jax.named_scope
SUBS = 2

def kernel(
    R, x_ref, g_ref, wu_in, wd_in,
    ig_ref, ru_ref, rd_ref,
    tok, wu, wd, act, slopes, s_t, h_t, part, r0, r1, r2, r3, ug, dg,
    send_sems, recv_sems, local_sems,
):
    z, f, c = lax.axis_index("rep"), lax.axis_index("fs"), lax.axis_index("tp")
    tl, D = x_ref.shape
    dl, fl = wu_in.shape
    h = fl // R
    pr = tl // 8
    half = 4 * pr
    sub = pr // SUBS
    steps = 2 * (R - 1)
    xx, yy = lax.rem(f, 2), lax.div(f, 2)
    fx, fy = yy * 2 + (1 - xx), (1 - yy) * 2 + xx
    f1 = fx * (1 - c) + fy * c
    f2 = fy * (1 - c) + fx * c
    f3 = 3 - f

    edge = jnp.minimum(z, R - 1 - z)
    far = jnp.where(z < R - 1 - z, 1, -1)
    inner = edge > 0
    outer = edge == 0

    def plane_at(slot):
        both = z + (slot // 2 + 1) * (2 * (slot % 2) - 1) * far
        return jnp.where(slot < 2 * edge, both, z + far * (slot + 1 - edge))

    near_first = [plane_at(slot) for slot in range(R - 1)]
    far_first = near_first[::-1]
    blocks = far_first + [z]

    def beyond(p):
        return jnp.logical_or(jnp.logical_and(p < z, z < R - 1), jnp.logical_and(p > z, z > 0))

    def past(p):
        return jnp.where(p < z, z + 1, z - 1)

    def toward(p):
        return jnp.where(p > z, z + 1, z - 1)

    send_names, recv_names = {}, {}

    def named(names, key, count):
        if key not in names:
            names[key] = sum(n for _, n in names.values()), count
        return names[key][0]

    def dev(zz=None, ff=None, cc=None):
        return {"rep": z if zz is None else zz, "fs": f if ff is None else ff, "tp": c if cc is None else cc}

    def remote(src, dst, device, group, key, index=0, count=1):
        return pltpu.make_async_remote_copy(
            src_ref=src, dst_ref=dst, send_sem=send_sems.at[named(send_names, group, 1)],
            recv_sem=recv_sems.at[named(recv_names, key, count) + index],
            device_id=device, device_id_type=MESH)

    def send(*args, **kw):
        remote(*args, **kw).start()

    def arrived(dst, key, index=0, count=1):
        pltpu.make_async_remote_copy(
            src_ref=dst, dst_ref=dst, send_sem=send_sems.at[0],
            recv_sem=recv_sems.at[named(recv_names, key, count) + index],
            device_id=dev(cc=1 - c), device_id_type=MESH).wait_recv()

    def sent(src, group):
        pltpu.make_async_remote_copy(
            src_ref=src, dst_ref=src, send_sem=send_sems.at[named(send_names, group, 1)],
            recv_sem=recv_sems.at[0], device_id=dev(cc=1 - c), device_id_type=MESH).wait_send()

    def sub_rows(zz, ff, n):
        return pl.ds(pl.multiple_of(zz * tl + (c * 4 + ff) * pr + n * sub, sub), sub)

    def rows(zz, ff, cc):
        return pl.ds(pl.multiple_of(zz * tl + (cc * 4 + ff) * pr, pr), pr)

    def core_rows(zz, cc):
        return pl.ds(pl.multiple_of(zz * tl + cc * half, half), half)

    def piece_rows(ff, cc):
        return pl.ds(pl.multiple_of((cc * 4 + ff) * pr, pr), pr)

    def up_cols(zz):
        return pl.ds(pl.multiple_of(zz * h, h), h)

    def d_block(zz):
        return pl.ds(pl.multiple_of(zz * dl, dl), dl)

    with SC("barrier"):
        barrier = pltpu.get_barrier_semaphore()
        near = [dev(zz=lax.rem(z + d, R)) for d in range(1, R)] + [dev(ff=fx), dev(ff=fy), dev(cc=1 - c)]
        for device in near:
            pl.semaphore_signal(barrier, inc=1, device_id=device, device_id_type=MESH)
        pl.semaphore_wait(barrier, len(near))

    TOK = dict(key="tok", count=2 * R)
    sources = (x_ref, g_ref)

    def send_own(a, to):
        copy = remote(sources[a].at[piece_rows(f, c), :], tok.at[a, rows(z, f, c), :],
                      dev(zz=to), "own", index=a * R + z, **TOK)
        copy.start()

    def send_up(p):
        send(wu_in.at[:, up_cols(p)], wu.at[d_block(z), :], dev(zz=p), "wu", "wu")

    def send_down(p):
        send(wd_in.at[up_cols(p), :], wd.at[:, d_block(z)], dev(zz=p), "wd", "wd")

    for a in (0, 1):
        send_own(a, near_first[0])
        send_own(a, near_first[1])

    @pl.when(outer)
    def _():
        send_up(near_first[0])
        send_up(near_first[1])
        send_down(near_first[1])
        send_down(near_first[0])
        send_up(near_first[2])

    @pl.when(inner)
    def _():
        for p in near_first[1:]:
            send_up(p)
        for p in near_first[1:]:
            send_down(p)

    own_rows = pl.ds(pl.multiple_of(z * tl, tl), tl)
    local = [
        pltpu.make_async_copy(x_ref, tok.at[0, own_rows, :], local_sems.at[0]),
        pltpu.make_async_copy(g_ref, tok.at[1, own_rows, :], local_sems.at[1]),
        pltpu.make_async_copy(wu_in.at[:, up_cols(z)], wu.at[d_block(z), :], local_sems.at[2]),
        pltpu.make_async_copy(wd_in.at[up_cols(z), :], wd.at[:, d_block(z)], local_sems.at[3]),
    ]
    for copy in local:
        copy.start()

    inner_order = [(0, 0), (0, 1), (0, 2), (1, 0), (1, 1), (1, 2)]
    outer_order = [(0, 0), (1, 0), (0, 1), (0, 2), (1, 1), (1, 2)]
    order = []
    for (ai, si), (ao, so) in zip(inner_order, outer_order):
        a = ai if ai == ao else jnp.where(inner, ai, ao)
        p = near_first[si] if si == so else jnp.where(inner, near_first[si], near_first[so])
        order.append((a, p))

    def spread(at, tag):
        group = tag + ("sent",)

        def first():
            mine = at(f, c)
            send(mine, mine, dev(ff=f1), group, tag + (1,))
            send(mine, mine, dev(ff=f2), group, tag + (2,))
            send(mine, mine, dev(cc=1 - c), group, tag + (4,))

        def second():
            p1, p2 = at(f1, c), at(f2, c)
            arrived(p1, tag + (1,))
            send(p1, p1, dev(ff=f2), group, tag + (3,))
            send(p1, p1, dev(cc=1 - c), group, tag + (4,))
            arrived(p2, tag + (2,))
            send(p2, p2, dev(cc=1 - c), group, tag + (4,))

        def third():
            p3 = at(f3, c)
            arrived(p3, tag + (3,))
            send(p3, p3, dev(cc=1 - c), group, tag + (4,))

        return first, second, third

    spreads = [
        spread(lambda ff, cc, a=a, p=p: tok.at[a, rows(p, ff, cc), :], ("tok", i))
        for i, (a, p) in enumerate(order)
    ]

    def forward(i):
        a, p = order[i]
        mine = tok.at[a, rows(p, f, c), :]
        return remote(mine, mine, dev(zz=near_first[0]), "fwd", index=a * R + p, **TOK)

    def take(i):
        a, p = order[i]
        arrived(tok.at[a, rows(p, f, c), :], index=a * R + p, **TOK)
        pl.when(jnp.logical_and(inner, p != near_first[0]))(forward(i).start)

    def first(i):
        with SC(f"first{i}"): spreads[i][0]()

    def second(i):
        with SC(f"second{i}"): spreads[i][1]()

    def third(i):
        with SC(f"third{i}"): spreads[i][2]()

    def last(i):
        a, p = order[i]
        with SC(f"last{i}"): arrived(tok.at[a, core_rows(p, 1 - c), :], ("tok", i, 4))

    def take_in(*which):
        @pl.when(inner)
        def _():
            for i in which:
                if i < steps:
                    with SC(f"takeI{i}"): take(i)

    def take_out(*which):
        @pl.when(outer)
        def _():
            for i in which:
                if i < steps:
                    with SC(f"takeO{i}"): take(i)

    take_in(0)
    take_out(0)
    first(0)
    take_in(1)
    take_out(1)
    first(1)
    take_in(2)
    second(0)
    take_out(2)
    first(2)
    take_in(3, 4)
    second(1)
    third(0)
    take_out(3)
    first(3)
    take_in(5)


    @pl.when(inner)
    def _():
        send_up(near_first[0])
        send_down(near_first[0])

    second(2)
    third(1)
    take_out(4)
    first(4)
    second(3)
    third(2)
    take_out(5)
    pl.when(outer)(functools.partial(send_down, near_first[2]))
    first(5)
    second(4)
    third(3)
    second(5)
    third(4)

    step = min(tl, 256)

    def up_block(p):
        @pl.loop(0, tl // step)
        def _(i):
            at = pl.ds(pl.multiple_of(p * tl + i * step, step), step)
            active = jnp.maximum(jnp.dot(tok[0, at, :], wu[...], preferred_element_type=F32), 0.0)
            act[at, :] = active
            h_t[:, at] = jnp.transpose(active * active).astype(BF16)

    for copy in local:
        copy.wait()
    others = (R - 1) * dl
    with SC("wuwait"): arrived(wu.at[pl.ds(0, others), :], "wu")
    with SC("upz"): up_block(z)
    for i in range(4):
        last(i)
    for slot in range(R - 1):
        with SC(f"up{slot}"): up_block(near_first[slot])
    third(5)
    last(4)
    last(5)

    def down_part(p):
        at = d_block(p)
        dg[:, at] = jnp.dot(h_t[...], tok[1, :, at], preferred_element_type=F32).astype(BF16)

    for p in near_first:
        with SC("downpart"): down_part(p)
        send(dg.at[:, d_block(p)], rd_ref.at[up_cols(z), :], dev(zz=p), "rd", "rd")
    with SC("downpartz"):
        down_part(z)
        rd_ref[up_cols(z), :] = dg[:, d_block(z)]

    with SC("wdwait"): arrived(wd.at[:, pl.ds(0, others)], "wd")

    def r0_rows(j, ff=None, n=0):
        if ff is None:
            return pl.ds(j * half, half)
        return pl.ds(pl.multiple_of(j * half + ff * pr + n * sub, sub), sub)

    def added(*terms):
        total = terms[0].astype(F32)
        for term in terms[1:]:
            total = total + term.astype(F32)
        return total.astype(BF16)

    def core_sum(j):
        p = blocks[j]
        arrived(r0.at[r0_rows(j), :], ("r0", j))
        for n in range(SUBS):
            for k, ff in ((1, f3), (0, f1)):
                at = sub_rows(p, ff, n)
                part[at, :] = added(part[at, :], r0[r0_rows(j, ff, n), :])
                send(part.at[at, :], r1.at[j, k, n], dev(ff=f1), "r1", ("r1", j, k, n))
        for ff in (f2, f):
            at = rows(p, ff, c)
            part[at, :] = added(part[at, :], r0[pl.ds(pl.multiple_of(j * half + ff * pr, pr), pr), :])

    def part_rows(at):
        value = 2.0 * act[at, :] * contract_last(tok[1, at, :], wd[...])
        slopes[at, :] = value.astype(BF16)
        part[at, :] = contract_last(slopes[at, :], wu[...]).astype(BF16)

    def slopes_turned():
        @pl.loop(0, R * tl // step)
        def _(i):
            at = pl.ds(pl.multiple_of(i * step, step), step)
            s_t[:, at] = jnp.transpose(slopes[at, :].astype(F32)).astype(BF16)

    def first_sum(j, n):
        at = sub_rows(blocks[j], f2, n)
        arrived(r1.at[j, 1, n], ("r1", j, 1, n))
        part[at, :] = added(part[at, :], r1[j, 1, n])
        send(part.at[at, :], r2.at[j, n], dev(ff=f2), "r2", ("r2", j, n))

    def second_sum(j, n):
        at = sub_rows(blocks[j], f, n)
        arrived(r1.at[j, 0, n], ("r1", j, 0, n))
        arrived(r2.at[j, n], ("r2", j, n))
        part[at, :] = added(part[at, :], r1[j, 0, n], r2[j, n])

    R3 = dict(key="r3", count=2 * R * SUBS)

    def r3_at(p, side, n):
        return (p * 2 + side) * SUBS + n

    def line_sum(j, n):
        p = blocks[j]
        at = sub_rows(p, f, n)
        side = jnp.where(p > z, 0, 1)

        @pl.when(beyond(p))
        def _():
            arrived(r3.at[p, side, n], index=r3_at(p, side, n), **R3)
            part[at, :] = added(part[at, :], r3[p, side, n])

        send(part.at[at, :], r3.at[p, side, n], dev(zz=toward(p)), "r3", index=r3_at(p, side, n), **R3)

    def own_sum(n):
        at = sub_rows(z, f, n)
        for side, there in ((0, z > 0), (1, z < R - 1)):
            @pl.when(there)
            def _(side=side):
                arrived(r3.at[z, side, n], index=r3_at(z, side, n), **R3)
                part[at, :] = added(part[at, :], r3[z, side, n])
        ig_ref[piece_sub(f, c, n), :] = part[at, :]

    def piece_sub(ff, cc, n):
        return pl.ds(pl.multiple_of((cc * 4 + ff) * pr + n * sub, sub), sub)

    def up_part(p):
        at = d_block(p)
        ug[at, :] = jnp.transpose(jnp.dot(s_t[...], tok[0, :, at], preferred_element_type=F32)).astype(BF16)

    def send_up_part(p):
        send(ug.at[d_block(p), :], ru_ref.at[:, up_cols(z)], dev(zz=p), "ru", "ru")

    def fs(j, n):
        with SC(f"fs{j}{n}"): first_sum(j, n)

    def ss(j, n):
        with SC(f"ss{j}{n}"): second_sum(j, n)
        if j < R - 1:
            @pl.when(outer)
            def _():
                with SC(f"lsO{j}{n}"): line_sum(j, n)

    def ls(j, n):
        @pl.when(inner)
        def _():
            with SC(f"lsI{j}{n}"): line_sum(j, n)

    def turn(slot):
        with SC("uppart"): up_part(far_first[slot])

    for j, p in enumerate(blocks):
        theirs = core_rows(p, 1 - c)
        with SC(f"slopesA{j}"): part_rows(theirs)
        send(part.at[theirs, :], r0.at[r0_rows(j), :], dev(cc=1 - c), "r0", ("r0", j))
        if j:
            with SC(f"core{j-1}"): core_sum(j - 1)
        if j == R - 1:
            fs(0, 0)
        with SC(f"slopesB{j}"): part_rows(core_rows(p, c))
    with SC(f"core{R-1}"): core_sum(R - 1)

    fs(0, 1)
    with SC("s_t"): slopes_turned()
    turn(0)
    pl.when(outer)(functools.partial(send_up_part, far_first[0]))
    ss(0, 0)
    fs(1, 0)
    turn(1)
    ss(0, 1)
    fs(1, 1)
    turn(2)
    pl.when(inner)(functools.partial(send_up_part, far_first[2]))
    ss(1, 0)
    with SC("uppartz"):
        up_part(z)
        ru_ref[:, up_cols(z)] = ug[d_block(z), :]
    fs(2, 0)
    ss(1, 1)
    ls(0, 0)
    fs(2, 1)
    ss(2, 0)
    ls(0, 1)
    fs(3, 0)
    ls(1, 0)
    ss(2, 1)

    @pl.when(outer)
    def _():
        send_up_part(far_first[1])
        send_up_part(far_first[2])

    ls(1, 1)

    @pl.when(inner)
    def _():
        send_up_part(far_first[0])
        send_up_part(far_first[1])

    fs(3, 1)
    ss(3, 0)
    ls(2, 0)
    ls(2, 1)

    gather = [spread(lambda ff, cc, n=n: ig_ref.at[piece_sub(ff, cc, n), :], ("ig", n)) for n in range(SUBS)]
    with SC("own0"): own_sum(0)
    gather[0][0]()
    ss(3, 1)
    with SC("own1"): own_sum(1)
    gather[1][0]()
    for k in (1, 2):
        for n in range(SUBS):
            with SC(f"ig{k}.{n}"): gather[n][k]()
    with SC("iglast"):
        for n in (0, 1):
            arrived(ig_ref.at[pl.ds(0, half // 2), :], ("ig", n, 4))

    with SC("rdwait"): arrived(rd_ref.at[pl.ds(0, (R - 1) * h), :], "rd")
    with SC("ruwait"): arrived(ru_ref.at[:, pl.ds(0, (R - 1) * h)], "ru")

    with SC("sendwait"):
        sent(part.at[pl.ds(0, 4 * pr), :], "own")
        pl.when(inner)(lambda: sent(part.at[pl.ds(0, 4 * pr), :], "fwd"))
        for i in range(steps):
            sent(part.at[pl.ds(0, 7 * pr), :], ("tok", i, "sent"))
        for n in (0, 1):
            sent(part.at[pl.ds(0, 7 * pr // 2), :], ("ig", n, "sent"))
        sent(wu.at[pl.ds(0, others), :], "wu")
        sent(wd.at[:, pl.ds(0, others)], "wd")
        sent(dg.at[:, pl.ds(0, others)], "rd")
        sent(ug.at[pl.ds(0, others), :], "ru")
        sent(r0, "r0")
        sent(r1, "r1")
        sent(r2, "r2")
        sent(part.at[pl.ds(0, (R - 1) * pr), :], "r3")
    for names, sems in ((send_names, send_sems), (recv_names, recv_sems)):
        assert sum(n for _, n in names.values()) == sems.shape[0], (names, sems.shape)


def in_planes(R, hidden_in, cotangent, w_up, w_down):
    tl, D = hidden_in.shape
    dl, fl = w_up.shape
    T, h, pr = tl * R, fl // R, tl // 8
    send_sems, recv_sems = 2 * R + 10, 10 * R - 4 + 5 * R * SUBS + R + 4 * SUBS
    vmem = pl.BlockSpec(memory_space=pltpu.VMEM)
    input_grad, up, down = pl.pallas_call(
        functools.partial(kernel, R),
        out_shape=(
            pltpu.VMEM((tl, D), BF16),
            pltpu.VMEM((dl, fl), BF16),
            pltpu.VMEM((fl, dl), BF16),
        ),
        in_specs=[pl.BlockSpec(memory_space=pl.ANY)] * 4,
        out_specs=(vmem, vmem, vmem),
        scratch_shapes=[
            pltpu.VMEM((2, T, D), BF16),
            pltpu.VMEM((D, h), BF16),
            pltpu.VMEM((h, D), BF16),
            pltpu.VMEM((T, h), F32),
            pltpu.VMEM((T, h), BF16),
            pltpu.VMEM((h, T), BF16),
            pltpu.VMEM((h, T), BF16),
            pltpu.VMEM((T, D), BF16),
            pltpu.VMEM((R * 4 * pr, D), BF16),
            pltpu.VMEM((R, 2, SUBS, pr // SUBS, D), BF16),
            pltpu.VMEM((R, SUBS, pr // SUBS, D), BF16),
            pltpu.VMEM((R, 2, SUBS, pr // SUBS, D), BF16),
            pltpu.VMEM((D, h), BF16),
            pltpu.VMEM((h, D), BF16),
            pltpu.SemaphoreType.DMA((send_sems,)),
            pltpu.SemaphoreType.DMA((recv_sems,)),
            pltpu.SemaphoreType.DMA((4,)),
        ],
        compiler_params=pltpu.CompilerParams(
            collective_id=0, has_side_effects=True, vmem_limit_bytes=58 * 1024 * 1024
        ),
    )(hidden_in, cotangent, w_up, w_down)
    return input_grad, up.astype(F32), down.astype(F32)


def solution(mesh):
    R, F, C = (mesh.shape[name] for name in ("rep", "fs", "tp"))
    body = functools.partial(in_planes, R) if (R, F, C) == (4, 4, 2) else plain
    return jax.shard_map(
        body,
        mesh=mesh,
        in_specs=(P("rep", None), P("rep", None), P("rep", ("fs", "tp")), P(("fs", "tp"), "rep")),
        out_specs=(P("rep", None), P("rep", ("fs", "tp")), P(("fs", "tp"), "rep")),
        check_vma=False,
    )
```

```python
import functools

import jax
import jax.numpy as jnp
from jax import lax
from jax.experimental import pallas as pl
from jax.experimental.pallas import tpu as pltpu
from jax.sharding import PartitionSpec as P

MESH = pl.DeviceIdType.MESH
BF16, F32 = jnp.bfloat16, jnp.float32


def contract_last(left, right):
    return lax.dot_general(left, right, (((1,), (1,)), ((), ())), preferred_element_type=F32)


def contract_first(left, right):
    return lax.dot_general(left, right, (((0,), (0,)), ((), ())), preferred_element_type=F32)


def plain(hidden_in, cotangent, w_up, w_down):
    up_full = lax.all_gather(w_up, "rep", axis=0, tiled=True)
    back_grad = contract_last(cotangent, lax.all_gather(w_down, "rep", axis=1, tiled=True))
    preact = jnp.dot(hidden_in, up_full, preferred_element_type=F32)
    active = jnp.maximum(preact, 0.0)
    hidden = (active * active).astype(BF16)
    slopes = (2.0 * active * back_grad).astype(BF16)
    grad_upper = lax.psum_scatter(
        contract_first(hidden_in, slopes).astype(BF16), "rep", scatter_dimension=0, tiled=True
    ).astype(F32)
    lower_rows = lax.psum_scatter(
        contract_first(cotangent, hidden).astype(BF16), "rep", scatter_dimension=0, tiled=True
    ).astype(F32)
    partial_sum = contract_last(slopes, up_full).astype(BF16)
    input_grad = lax.psum(partial_sum, ("fs", "tp")).astype(F32).astype(BF16)
    return (input_grad, grad_upper, lower_rows.T)


SC = jax.named_scope
SUBS, CHUNKS = 2, 4

def kernel(
    R, x_ref, g_ref, wu_in, wd_in,
    ig_ref, ru_ref, down_ref,
    rd_ref, stage, tok, wu, wd, act, slopes, s_t, h_t, part, r0, r1, r2, r3, ug, dg,
    send_sems, recv_sems, local_sems,
):
    z, f, c = lax.axis_index("rep"), lax.axis_index("fs"), lax.axis_index("tp")
    tl, D = x_ref.shape
    dl, fl = wu_in.shape
    h = fl // R
    pr = tl // 8
    half = 4 * pr
    sub = pr // SUBS
    steps = 2 * (R - 1)
    xx, yy = lax.rem(f, 2), lax.div(f, 2)
    fx, fy = yy * 2 + (1 - xx), (1 - yy) * 2 + xx
    f1 = fx * (1 - c) + fy * c
    f2 = fy * (1 - c) + fx * c
    f3 = 3 - f

    edge = jnp.minimum(z, R - 1 - z)
    far = jnp.where(z < R - 1 - z, 1, -1)
    inner = edge > 0
    outer = edge == 0

    def plane_at(slot):
        both = z + (slot // 2 + 1) * (2 * (slot % 2) - 1) * far
        return jnp.where(slot < 2 * edge, both, z + far * (slot + 1 - edge))

    near_first = [plane_at(slot) for slot in range(R - 1)]
    far_first = near_first[::-1]
    blocks = far_first + [z]

    def beyond(p):
        return jnp.logical_or(jnp.logical_and(p < z, z < R - 1), jnp.logical_and(p > z, z > 0))

    def past(p):
        return jnp.where(p < z, z + 1, z - 1)

    def toward(p):
        return jnp.where(p > z, z + 1, z - 1)

    send_names, recv_names = {}, {}

    def named(names, key, count):
        if key not in names:
            names[key] = sum(n for _, n in names.values()), count
        return names[key][0]

    def dev(zz=None, ff=None, cc=None):
        return {"rep": z if zz is None else zz, "fs": f if ff is None else ff, "tp": c if cc is None else cc}

    def remote(src, dst, device, group, key, index=0, count=1):
        return pltpu.make_async_remote_copy(
            src_ref=src, dst_ref=dst, send_sem=send_sems.at[named(send_names, group, 1)],
            recv_sem=recv_sems.at[named(recv_names, key, count) + index],
            device_id=device, device_id_type=MESH)

    def send(*args, **kw):
        remote(*args, **kw).start()

    def arrived(dst, key, index=0, count=1):
        pltpu.make_async_remote_copy(
            src_ref=dst, dst_ref=dst, send_sem=send_sems.at[0],
            recv_sem=recv_sems.at[named(recv_names, key, count) + index],
            device_id=dev(cc=1 - c), device_id_type=MESH).wait_recv()

    def sent(src, group):
        pltpu.make_async_remote_copy(
            src_ref=src, dst_ref=src, send_sem=send_sems.at[named(send_names, group, 1)],
            recv_sem=recv_sems.at[0], device_id=dev(cc=1 - c), device_id_type=MESH).wait_send()

    def sub_rows(zz, ff, n):
        return pl.ds(pl.multiple_of(zz * tl + (c * 4 + ff) * pr + n * sub, sub), sub)

    def rows(zz, ff, cc):
        return pl.ds(pl.multiple_of(zz * tl + (cc * 4 + ff) * pr, pr), pr)

    def core_rows(zz, cc):
        return pl.ds(pl.multiple_of(zz * tl + cc * half, half), half)

    def piece_rows(ff, cc):
        return pl.ds(pl.multiple_of((cc * 4 + ff) * pr, pr), pr)

    def up_cols(zz):
        return pl.ds(pl.multiple_of(zz * h, h), h)

    def d_block(zz):
        return pl.ds(pl.multiple_of(zz * dl, dl), dl)

    sources = (x_ref, g_ref)
    staged = [
        pltpu.make_async_copy(sources[a].at[piece_rows(f, c), :], stage.at[a], local_sems.at[a])
        for a in (0, 1)
    ]
    for copy in staged:
        copy.start()

    with SC("barrier"):
        barrier = pltpu.get_barrier_semaphore()
        near = [dev(zz=lax.rem(z + d, R)) for d in range(1, R)] + [dev(ff=fx), dev(ff=fy), dev(cc=1 - c)]
        for device in near:
            pl.semaphore_signal(barrier, inc=1, device_id=device, device_id_type=MESH)
        pl.semaphore_wait(barrier, len(near))

    TOK = dict(key="tok", count=2 * R)

    def send_own(a, to):
        send(stage.at[a], tok.at[a, rows(z, f, c), :], dev(zz=to), "early", index=a * R + z, **TOK)

    def send_up(p):
        send(wu_in.at[:, up_cols(p)], wu.at[d_block(z), :], dev(zz=p), "wu", "wu")

    def send_down(p):
        send(wd_in.at[up_cols(p), :], wd.at[:, d_block(z)], dev(zz=p), "wd", "wd")

    for a in (0, 1):
        staged[a].wait()
        send_own(a, near_first[0])
        send_own(a, near_first[1])

    @pl.when(outer)
    def _():
        send_up(near_first[0])
        send_up(near_first[1])
        send_down(near_first[1])
        send_down(near_first[0])
        send_up(near_first[2])

    @pl.when(inner)
    def _():
        for p in near_first[1:]:
            send_up(p)
        for p in near_first[1:]:
            send_down(p)

    own_rows = pl.ds(pl.multiple_of(z * tl, tl), tl)
    local = [
        pltpu.make_async_copy(x_ref, tok.at[0, own_rows, :], local_sems.at[2]),
        pltpu.make_async_copy(g_ref, tok.at[1, own_rows, :], local_sems.at[2]),
        pltpu.make_async_copy(wu_in.at[:, up_cols(z)], wu.at[d_block(z), :], local_sems.at[3]),
        pltpu.make_async_copy(wd_in.at[up_cols(z), :], wd.at[:, d_block(z)], local_sems.at[4]),
    ]
    for copy in local:
        copy.start()

    inner_order = [(0, 0), (0, 1), (0, 2), (1, 0), (1, 1), (1, 2)]
    outer_order = [(0, 0), (1, 0), (0, 1), (0, 2), (1, 1), (1, 2)]
    order = []
    for (ai, si), (ao, so) in zip(inner_order, outer_order):
        a = ai if ai == ao else jnp.where(inner, ai, ao)
        p = near_first[si] if si == so else jnp.where(inner, near_first[si], near_first[so])
        order.append((a, p))

    def spread(at, tag, group):

        def first():
            mine = at(f, c)
            send(mine, mine, dev(ff=f1), group, tag + (1,))
            send(mine, mine, dev(ff=f2), group, tag + (2,))
            send(mine, mine, dev(cc=1 - c), group, tag + (4,))

        def second():
            p1, p2 = at(f1, c), at(f2, c)
            arrived(p1, tag + (1,))
            send(p1, p1, dev(ff=f2), group, tag + (3,))
            send(p1, p1, dev(cc=1 - c), group, tag + (4,))
            arrived(p2, tag + (2,))
            send(p2, p2, dev(cc=1 - c), group, tag + (4,))

        def third():
            p3 = at(f3, c)
            arrived(p3, tag + (3,))
            send(p3, p3, dev(cc=1 - c), group, tag + (4,))

        return first, second, third

    spreads = [
        spread(lambda ff, cc, a=a, p=p: tok.at[a, rows(p, ff, cc), :], ("tok", i), "early")
        for i, (a, p) in enumerate(order)
    ]

    def forward(i):
        a, p = order[i]
        mine = tok.at[a, rows(p, f, c), :]
        return remote(mine, mine, dev(zz=near_first[0]), "fwd", index=a * R + p, **TOK)

    def take(i):
        a, p = order[i]
        arrived(tok.at[a, rows(p, f, c), :], index=a * R + p, **TOK)
        pl.when(jnp.logical_and(inner, p != near_first[0]))(forward(i).start)

    def first(i):
        with SC(f"first{i}"): spreads[i][0]()

    def second(i):
        with SC(f"second{i}"): spreads[i][1]()

    def third(i):
        with SC(f"third{i}"): spreads[i][2]()

    def last(i):
        a, p = order[i]
        with SC(f"last{i}"): arrived(tok.at[a, core_rows(p, 1 - c), :], ("tok", i, 4))

    def take_in(*which):
        @pl.when(inner)
        def _():
            for i in which:
                if i < steps:
                    with SC(f"takeI{i}"): take(i)

    def take_out(*which):
        @pl.when(outer)
        def _():
            for i in which:
                if i < steps:
                    with SC(f"takeO{i}"): take(i)

    take_in(0)
    take_out(0)
    first(0)
    take_in(1)
    take_out(1)
    first(1)
    take_in(2)
    second(0)
    take_out(2)
    first(2)
    take_in(3, 4)
    second(1)
    third(0)
    take_out(3)
    first(3)
    take_in(5)


    @pl.when(inner)
    def _():
        send_up(near_first[0])
        send_down(near_first[0])

    second(2)
    third(1)
    take_out(4)
    first(4)
    second(3)
    third(2)
    take_out(5)
    pl.when(outer)(functools.partial(send_down, near_first[2]))
    first(5)
    second(4)
    third(3)
    second(5)
    third(4)

    step = min(tl, 256)

    def up_block(p):
        @pl.loop(0, tl // step)
        def _(i):
            at = pl.ds(pl.multiple_of(p * tl + i * step, step), step)
            active = jnp.maximum(jnp.dot(tok[0, at, :], wu[...], preferred_element_type=F32), 0.0)
            act[at, :] = active
            h_t[:, at] = jnp.transpose(active * active).astype(BF16)

    own_tokens = tok.at[:, own_rows, :]
    pltpu.make_async_copy(own_tokens, own_tokens, local_sems.at[2]).wait()
    for copy in local[2:]:
        copy.wait()
    others = (R - 1) * dl
    with SC("wuwait"): arrived(wu.at[pl.ds(0, others), :], "wu")
    with SC("upz"): up_block(z)
    for i in range(4):
        last(i)
    for slot in range(R - 1):
        with SC(f"up{slot}"): up_block(near_first[slot])
    third(5)
    last(4)
    last(5)

    def down_part(p):
        at = d_block(p)
        dg[:, at] = jnp.dot(h_t[...], tok[1, :, at], preferred_element_type=F32).astype(BF16)

    for p in near_first:
        with SC("downpart"): down_part(p)
        send(dg.at[:, d_block(p)], rd_ref.at[up_cols(z), :], dev(zz=p), "rd", "rd")
    with SC("downpartz"):
        down_part(z)
        rd_ref[up_cols(z), :] = dg[:, d_block(z)]

    with SC("wdwait"): arrived(wd.at[:, pl.ds(0, others)], "wd")

    def r0_rows(j, ff=None, n=0):
        if ff is None:
            return pl.ds(j * half, half)
        return pl.ds(pl.multiple_of(j * half + ff * pr + n * sub, sub), sub)

    def added(*terms):
        total = terms[0].astype(F32)
        for term in terms[1:]:
            total = total + term.astype(F32)
        return total.astype(BF16)

    def core_sum(j):
        p = blocks[j]
        arrived(r0.at[r0_rows(j), :], ("r0", j))
        for n in range(SUBS):
            for k, ff in ((1, f3), (0, f1)):
                at = sub_rows(p, ff, n)
                part[at, :] = added(part[at, :], r0[r0_rows(j, ff, n), :])
                send(part.at[at, :], r1.at[j, k, n], dev(ff=f1), "late", ("r1", j, k, n))
        for ff in (f2, f):
            at = rows(p, ff, c)
            part[at, :] = added(part[at, :], r0[pl.ds(pl.multiple_of(j * half + ff * pr, pr), pr), :])

    def part_rows(at):
        value = 2.0 * act[at, :] * contract_last(tok[1, at, :], wd[...])
        slopes[at, :] = value.astype(BF16)
        part[at, :] = contract_last(slopes[at, :], wu[...]).astype(BF16)

    def slopes_turned():
        @pl.loop(0, R * tl // step)
        def _(i):
            at = pl.ds(pl.multiple_of(i * step, step), step)
            s_t[:, at] = jnp.transpose(slopes[at, :].astype(F32)).astype(BF16)

    def first_sum(j, n):
        at = sub_rows(blocks[j], f2, n)
        arrived(r1.at[j, 1, n], ("r1", j, 1, n))
        part[at, :] = added(part[at, :], r1[j, 1, n])
        send(part.at[at, :], r2.at[j, n], dev(ff=f2), "late", ("r2", j, n))

    def second_sum(j, n):
        at = sub_rows(blocks[j], f, n)
        arrived(r1.at[j, 0, n], ("r1", j, 0, n))
        arrived(r2.at[j, n], ("r2", j, n))
        part[at, :] = added(part[at, :], r1[j, 0, n], r2[j, n])

    R3 = dict(key="r3", count=2 * R * SUBS)

    def r3_at(p, side, n):
        return (p * 2 + side) * SUBS + n

    def line_sum(j, n):
        p = blocks[j]
        at = sub_rows(p, f, n)
        side = jnp.where(p > z, 0, 1)

        @pl.when(beyond(p))
        def _():
            arrived(r3.at[p, side, n], index=r3_at(p, side, n), **R3)
            part[at, :] = added(part[at, :], r3[p, side, n])

        send(part.at[at, :], r3.at[p, side, n], dev(zz=toward(p)), "late", index=r3_at(p, side, n), **R3)

    def own_sum(n):
        at = sub_rows(z, f, n)
        for side, there in ((0, z > 0), (1, z < R - 1)):
            @pl.when(there)
            def _(side=side):
                arrived(r3.at[z, side, n], index=r3_at(z, side, n), **R3)
                part[at, :] = added(part[at, :], r3[z, side, n])
        ig_ref[piece_sub(f, c, n), :] = part[at, :]

    def piece_sub(ff, cc, n):
        return pl.ds(pl.multiple_of((cc * 4 + ff) * pr + n * sub, sub), sub)

    def up_part(p):
        at = d_block(p)
        ug[at, :] = jnp.transpose(jnp.dot(s_t[...], tok[0, :, at], preferred_element_type=F32)).astype(BF16)

    def send_up_part(p):
        send(ug.at[d_block(p), :], ru_ref.at[:, up_cols(z)], dev(zz=p), "ru", "ru")

    def fs(j, n):
        with SC(f"fs{j}{n}"): first_sum(j, n)

    def ss(j, n):
        with SC(f"ss{j}{n}"): second_sum(j, n)
        if j < R - 1:
            @pl.when(outer)
            def _():
                with SC(f"lsO{j}{n}"): line_sum(j, n)

    def ls(j, n):
        @pl.when(inner)
        def _():
            with SC(f"lsI{j}{n}"): line_sum(j, n)

    def turn(slot):
        with SC("uppart"): up_part(far_first[slot])

    for j, p in enumerate(blocks):
        theirs = core_rows(p, 1 - c)
        with SC(f"slopesA{j}"): part_rows(theirs)
        send(part.at[theirs, :], r0.at[r0_rows(j), :], dev(cc=1 - c), "late", ("r0", j))
        if j:
            with SC(f"core{j-1}"): core_sum(j - 1)
        if j == R - 1:
            fs(0, 0)
        with SC(f"slopesB{j}"): part_rows(core_rows(p, c))
    with SC(f"core{R-1}"): core_sum(R - 1)

    fs(0, 1)
    with SC("s_t"): slopes_turned()
    turn(0)
    pl.when(outer)(functools.partial(send_up_part, far_first[0]))
    ss(0, 0)
    fs(1, 0)
    turn(1)
    ss(0, 1)
    fs(1, 1)
    turn(2)
    pl.when(inner)(functools.partial(send_up_part, far_first[2]))
    ss(1, 0)
    with SC("uppartz"):
        up_part(z)
        ru_ref[:, up_cols(z)] = ug[d_block(z), :]
    fs(2, 0)
    ss(1, 1)
    ls(0, 0)
    fs(2, 1)
    ss(2, 0)
    ls(0, 1)
    fs(3, 0)
    ls(1, 0)
    ss(2, 1)

    @pl.when(outer)
    def _():
        send_up_part(far_first[1])
        send_up_part(far_first[2])

    ls(1, 1)

    @pl.when(inner)
    def _():
        send_up_part(far_first[0])
        send_up_part(far_first[1])

    fs(3, 1)
    ss(3, 0)
    ls(2, 0)
    ls(2, 1)

    with SC("earlysent"):
        sent(tok.at[:, pl.ds(0, (7 * R - 5) * pr), :], "early")
        pl.when(inner)(lambda: sent(part.at[pl.ds(0, 4 * pr), :], "fwd"))
        sent(wu.at[pl.ds(0, others), :], "wu")
        sent(wd.at[:, pl.ds(0, others)], "wd")
        sent(dg.at[:, pl.ds(0, others)], "rd")
    with SC("rdwait"):
        arrived(rd_ref.at[pl.ds(0, (R - 1) * h), :], "rd")
        down_ref[...] = rd_ref[...].astype(F32)

    gather = [spread(lambda ff, cc, n=n: ig_ref.at[piece_sub(ff, cc, n), :], ("ig", n), "late") for n in range(SUBS)]
    with SC("own0"): own_sum(0)
    gather[0][0]()
    ss(3, 1)
    with SC("own1"): own_sum(1)
    gather[1][0]()
    for k in (1, 2):
        for n in range(SUBS):
            with SC(f"ig{k}.{n}"): gather[n][k]()
    with SC("iglast"):
        for n in (0, 1):
            arrived(ig_ref.at[pl.ds(0, half // 2), :], ("ig", n, 4))

    with SC("ruwait"): arrived(ru_ref.at[:, pl.ds(0, (R - 1) * h)], "ru")

    with SC("sendwait"):
        sent(ug.at[pl.ds(0, others), :], "ru")
        sent(tok.at[:, pl.ds(0, (4 * R + 3) * pr), :], "late")
    for names, sems in ((send_names, send_sems), (recv_names, recv_sems)):
        assert sum(n for _, n in names.values()) == sems.shape[0], (names, sems.shape)


def in_planes(R, hidden_in, cotangent, w_up, w_down):
    tl, D = hidden_in.shape
    dl, fl = w_up.shape
    T, h, pr = tl * R, fl // R, tl // 8
    send_sems, recv_sems = 7, 10 * R - 4 + 5 * R * SUBS + R + 4 * SUBS
    vmem = pl.BlockSpec(memory_space=pltpu.VMEM)
    input_grad, up, down = pl.pallas_call(
        functools.partial(kernel, R),
        out_shape=(
            pltpu.VMEM((tl, D), BF16),
            pltpu.VMEM((dl, fl), BF16),
            pltpu.VMEM((fl, dl), F32),
        ),
        in_specs=[pl.BlockSpec(memory_space=pl.ANY)] * 4,
        out_specs=(vmem, vmem, vmem),
        scratch_shapes=[
            pltpu.VMEM((fl, dl), BF16),
            pltpu.VMEM((2, pr, D), BF16),
            pltpu.VMEM((2, T, D), BF16),
            pltpu.VMEM((D, h), BF16),
            pltpu.VMEM((h, D), BF16),
            pltpu.VMEM((T, h), F32),
            pltpu.VMEM((T, h), BF16),
            pltpu.VMEM((h, T), BF16),
            pltpu.VMEM((h, T), BF16),
            pltpu.VMEM((T, D), BF16),
            pltpu.VMEM((R * 4 * pr, D), BF16),
            pltpu.VMEM((R, 2, SUBS, pr // SUBS, D), BF16),
            pltpu.VMEM((R, SUBS, pr // SUBS, D), BF16),
            pltpu.VMEM((R, 2, SUBS, pr // SUBS, D), BF16),
            pltpu.VMEM((D, h), BF16),
            pltpu.VMEM((h, D), BF16),
            pltpu.SemaphoreType.DMA((send_sems,)),
            pltpu.SemaphoreType.DMA((recv_sems,)),
            pltpu.SemaphoreType.DMA((5,)),
        ],
        compiler_params=pltpu.CompilerParams(
            collective_id=0, has_side_effects=True, vmem_limit_bytes=58 * 1024 * 1024
        ),
    )(hidden_in, cotangent, w_up, w_down)
    return written_out(input_grad, up, down)


def write_out(ig_ref, up_ref, down_ref, ig_out, up_out, down_out, wide, sems):
    copies = [
        pltpu.make_async_copy(ig_ref, ig_out, sems.at[0]),
        pltpu.make_async_copy(down_ref, down_out, sems.at[1]),
    ]
    for copy in copies:
        copy.start()
    n = up_ref.shape[0] // CHUNKS
    for i in range(CHUNKS):
        at = pl.ds(i * n, n)
        wide[at, :] = up_ref[at, :].astype(F32)
        copies.append(pltpu.make_async_copy(wide.at[at, :], up_out.at[at, :], sems.at[2 + i]))
        copies[-1].start()
    for copy in copies:
        copy.wait()


def written_out(input_grad, up, down):
    vmem = pl.BlockSpec(memory_space=pltpu.VMEM)
    there = [pltpu.with_memory_space_constraint(x, pltpu.VMEM) for x in (input_grad, up, down)]
    return pl.pallas_call(
        write_out,
        out_shape=(
            jax.ShapeDtypeStruct(input_grad.shape, BF16),
            jax.ShapeDtypeStruct(up.shape, F32),
            jax.ShapeDtypeStruct(down.shape, F32),
        ),
        in_specs=[vmem] * 3,
        out_specs=[pl.BlockSpec(memory_space=pl.ANY)] * 3,
        scratch_shapes=[pltpu.VMEM(up.shape, F32), pltpu.SemaphoreType.DMA((2 + CHUNKS,))],
        compiler_params=pltpu.CompilerParams(vmem_limit_bytes=8 * 1024 * 1024),
    )(*there)


def solution(mesh):
    R, F, C = (mesh.shape[name] for name in ("rep", "fs", "tp"))
    body = functools.partial(in_planes, R) if (R, F, C) == (4, 4, 2) else plain
    return jax.shard_map(
        body,
        mesh=mesh,
        in_specs=(P("rep", None), P("rep", None), P("rep", ("fs", "tp")), P(("fs", "tp"), "rep")),
        out_specs=(P("rep", None), P("rep", ("fs", "tp")), P(("fs", "tp"), "rep")),
        check_vma=False,
    )
```

```python
import functools

import jax
import jax.numpy as jnp
from jax import lax
from jax.experimental import pallas as pl
from jax.experimental.pallas import tpu as pltpu
from jax.sharding import PartitionSpec as P

MESH = pl.DeviceIdType.MESH
BF16, F32 = jnp.bfloat16, jnp.float32


def contract_last(left, right):
    return lax.dot_general(left, right, (((1,), (1,)), ((), ())), preferred_element_type=F32)


def contract_first(left, right):
    return lax.dot_general(left, right, (((0,), (0,)), ((), ())), preferred_element_type=F32)


def plain(hidden_in, cotangent, w_up, w_down):
    up_full = lax.all_gather(w_up, "rep", axis=0, tiled=True)
    back_grad = contract_last(cotangent, lax.all_gather(w_down, "rep", axis=1, tiled=True))
    preact = jnp.dot(hidden_in, up_full, preferred_element_type=F32)
    active = jnp.maximum(preact, 0.0)
    hidden = (active * active).astype(BF16)
    slopes = (2.0 * active * back_grad).astype(BF16)
    grad_upper = lax.psum_scatter(
        contract_first(hidden_in, slopes).astype(BF16), "rep", scatter_dimension=0, tiled=True
    ).astype(F32)
    lower_rows = lax.psum_scatter(
        contract_first(cotangent, hidden).astype(BF16), "rep", scatter_dimension=0, tiled=True
    ).astype(F32)
    partial_sum = contract_last(slopes, up_full).astype(BF16)
    input_grad = lax.psum(partial_sum, ("fs", "tp")).astype(F32).astype(BF16)
    return (input_grad, grad_upper, lower_rows.T)


SC = jax.named_scope
SUBS, PIECES, CHUNKS, PARTS = 2, 4, 8, 2

def kernel(
    R, x_ref, g_ref, wu_in, wd_in,
    ig_ref, ru_ref, down_ref,
    rd_ref, stage, tok, wu, wd, act, slopes, s_t, h_t, part, r0, r1, r2, r3, ug, dg,
    send_sems, recv_sems, local_sems,
):
    z, f, c = lax.axis_index("rep"), lax.axis_index("fs"), lax.axis_index("tp")
    tl, D = x_ref.shape
    dl, fl = wu_in.shape
    h = fl // R
    pr = tl // 8
    half = 4 * pr
    sub = pr // SUBS
    steps = 2 * (R - 1)
    xx, yy = lax.rem(f, 2), lax.div(f, 2)
    fx, fy = yy * 2 + (1 - xx), (1 - yy) * 2 + xx
    f1 = fx * (1 - c) + fy * c
    f2 = fy * (1 - c) + fx * c
    f3 = 3 - f

    edge = jnp.minimum(z, R - 1 - z)
    far = jnp.where(z < R - 1 - z, 1, -1)
    inner = edge > 0
    outer = edge == 0

    def plane_at(slot):
        both = z + (slot // 2 + 1) * (2 * (slot % 2) - 1) * far
        return jnp.where(slot < 2 * edge, both, z + far * (slot + 1 - edge))

    near_first = [plane_at(slot) for slot in range(R - 1)]
    far_first = near_first[::-1]
    blocks = far_first + [z]

    def beyond(p):
        return jnp.logical_or(jnp.logical_and(p < z, z < R - 1), jnp.logical_and(p > z, z > 0))

    def past(p):
        return jnp.where(p < z, z + 1, z - 1)

    def toward(p):
        return jnp.where(p > z, z + 1, z - 1)

    send_names, recv_names = {}, {}

    def named(names, key, count):
        if key not in names:
            names[key] = sum(n for _, n in names.values()), count
        return names[key][0]

    def dev(zz=None, ff=None, cc=None):
        return {"rep": z if zz is None else zz, "fs": f if ff is None else ff, "tp": c if cc is None else cc}

    def remote(src, dst, device, group, key, index=0, count=1):
        return pltpu.make_async_remote_copy(
            src_ref=src, dst_ref=dst, send_sem=send_sems.at[named(send_names, group, 1)],
            recv_sem=recv_sems.at[named(recv_names, key, count) + index],
            device_id=device, device_id_type=MESH)

    def send(*args, **kw):
        remote(*args, **kw).start()

    def arrived(dst, key, index=0, count=1):
        pltpu.make_async_remote_copy(
            src_ref=dst, dst_ref=dst, send_sem=send_sems.at[0],
            recv_sem=recv_sems.at[named(recv_names, key, count) + index],
            device_id=dev(cc=1 - c), device_id_type=MESH).wait_recv()

    def sent(src, group):
        pltpu.make_async_remote_copy(
            src_ref=src, dst_ref=src, send_sem=send_sems.at[named(send_names, group, 1)],
            recv_sem=recv_sems.at[0], device_id=dev(cc=1 - c), device_id_type=MESH).wait_send()

    def sub_rows(zz, ff, n):
        return pl.ds(pl.multiple_of(zz * tl + (c * 4 + ff) * pr + n * sub, sub), sub)

    def rows(zz, ff, cc):
        return pl.ds(pl.multiple_of(zz * tl + (cc * 4 + ff) * pr, pr), pr)

    def core_rows(zz, cc):
        return pl.ds(pl.multiple_of(zz * tl + cc * half, half), half)

    def piece_rows(ff, cc):
        return pl.ds(pl.multiple_of((cc * 4 + ff) * pr, pr), pr)

    def up_cols(zz):
        return pl.ds(pl.multiple_of(zz * h, h), h)

    def d_block(zz):
        return pl.ds(pl.multiple_of(zz * dl, dl), dl)

    sources = (x_ref, g_ref)
    staged = [
        pltpu.make_async_copy(sources[a].at[piece_rows(f, c), :], stage.at[a], local_sems.at[a])
        for a in (0, 1)
    ]
    for copy in staged:
        copy.start()

    with SC("barrier"):
        barrier = pltpu.get_barrier_semaphore()
        near = [dev(zz=lax.rem(z + d, R)) for d in range(1, R)] + [dev(ff=fx), dev(ff=fy), dev(cc=1 - c)]
        for device in near:
            pl.semaphore_signal(barrier, inc=1, device_id=device, device_id_type=MESH)
        pl.semaphore_wait(barrier, len(near))

    TOK = dict(key="tok", count=2 * R)

    def send_own(a, to):
        send(stage.at[a], tok.at[a, rows(z, f, c), :], dev(zz=to), "early", index=a * R + z, **TOK)

    def send_up(p):
        send(wu_in.at[:, up_cols(p)], wu.at[d_block(z), :], dev(zz=p), "wu", "wu")

    def send_down(p):
        send(wd_in.at[up_cols(p), :], wd.at[:, d_block(z)], dev(zz=p), "wd", "wd")

    for a in (0, 1):
        staged[a].wait()
        send_own(a, near_first[0])
        send_own(a, near_first[1])

    @pl.when(outer)
    def _():
        send_up(near_first[0])
        send_up(near_first[1])
        send_down(near_first[1])
        send_down(near_first[0])
        send_up(near_first[2])

    @pl.when(inner)
    def _():
        for p in near_first[1:]:
            send_up(p)
        for p in near_first[1:]:
            send_down(p)

    own_rows = pl.ds(pl.multiple_of(z * tl, tl), tl)
    local = [
        pltpu.make_async_copy(x_ref, tok.at[0, own_rows, :], local_sems.at[2]),
        pltpu.make_async_copy(g_ref, tok.at[1, own_rows, :], local_sems.at[2]),
        pltpu.make_async_copy(wu_in.at[:, up_cols(z)], wu.at[d_block(z), :], local_sems.at[3]),
        pltpu.make_async_copy(wd_in.at[up_cols(z), :], wd.at[:, d_block(z)], local_sems.at[4]),
    ]
    for copy in local:
        copy.start()

    inner_order = [(0, 0), (0, 1), (0, 2), (1, 0), (1, 1), (1, 2)]
    outer_order = [(0, 0), (1, 0), (0, 1), (0, 2), (1, 1), (1, 2)]
    order = []
    for (ai, si), (ao, so) in zip(inner_order, outer_order):
        a = ai if ai == ao else jnp.where(inner, ai, ao)
        p = near_first[si] if si == so else jnp.where(inner, near_first[si], near_first[so])
        order.append((a, p))

    def spread(at, tag, group):

        def first():
            mine = at(f, c)
            send(mine, mine, dev(ff=f1), group, tag + (1,))
            send(mine, mine, dev(ff=f2), group, tag + (2,))
            send(mine, mine, dev(cc=1 - c), group, tag + (4,))

        def second():
            p1, p2 = at(f1, c), at(f2, c)
            arrived(p1, tag + (1,))
            send(p1, p1, dev(ff=f2), group, tag + (3,))
            send(p1, p1, dev(cc=1 - c), group, tag + (4,))
            arrived(p2, tag + (2,))
            send(p2, p2, dev(cc=1 - c), group, tag + (4,))

        def third():
            p3 = at(f3, c)
            arrived(p3, tag + (3,))
            send(p3, p3, dev(cc=1 - c), group, tag + (4,))

        return first, second, third

    spreads = [
        spread(lambda ff, cc, a=a, p=p: tok.at[a, rows(p, ff, cc), :], ("tok", i), "early")
        for i, (a, p) in enumerate(order)
    ]

    def forward(i):
        a, p = order[i]
        mine = tok.at[a, rows(p, f, c), :]
        return remote(mine, mine, dev(zz=near_first[0]), "fwd", index=a * R + p, **TOK)

    def take(i):
        a, p = order[i]
        arrived(tok.at[a, rows(p, f, c), :], index=a * R + p, **TOK)
        pl.when(jnp.logical_and(inner, p != near_first[0]))(forward(i).start)

    def first(i):
        with SC(f"first{i}"): spreads[i][0]()

    def second(i):
        with SC(f"second{i}"): spreads[i][1]()

    def third(i):
        with SC(f"third{i}"): spreads[i][2]()

    def last(i):
        a, p = order[i]
        with SC(f"last{i}"): arrived(tok.at[a, core_rows(p, 1 - c), :], ("tok", i, 4))

    def take_in(*which):
        @pl.when(inner)
        def _():
            for i in which:
                if i < steps:
                    with SC(f"takeI{i}"): take(i)

    def take_out(*which):
        @pl.when(outer)
        def _():
            for i in which:
                if i < steps:
                    with SC(f"takeO{i}"): take(i)

    take_in(0)
    take_out(0)
    first(0)
    take_in(1)
    take_out(1)
    first(1)
    take_in(2)
    second(0)
    take_out(2)
    first(2)
    take_in(3, 4)
    second(1)
    third(0)
    take_out(3)
    first(3)
    take_in(5)


    @pl.when(inner)
    def _():
        send_up(near_first[0])
        send_down(near_first[0])

    second(2)
    third(1)
    take_out(4)
    first(4)
    second(3)
    third(2)
    take_out(5)
    pl.when(outer)(functools.partial(send_down, near_first[2]))
    first(5)
    second(4)
    third(3)
    second(5)
    third(4)

    step = min(tl, 256)

    def up_block(p):
        @pl.loop(0, tl // step)
        def _(i):
            at = pl.ds(pl.multiple_of(p * tl + i * step, step), step)
            active = jnp.maximum(jnp.dot(tok[0, at, :], wu[...], preferred_element_type=F32), 0.0)
            act[at, :] = active
            h_t[:, at] = jnp.transpose(active * active).astype(BF16)

    own_tokens = tok.at[:, own_rows, :]
    pltpu.make_async_copy(own_tokens, own_tokens, local_sems.at[2]).wait()
    for copy in local[2:]:
        copy.wait()
    others = (R - 1) * dl
    with SC("wuwait"): arrived(wu.at[pl.ds(0, others), :], "wu")
    with SC("upz"): up_block(z)
    for i in range(4):
        last(i)
    for slot in range(R - 1):
        with SC(f"up{slot}"): up_block(near_first[slot])
    third(5)
    last(4)
    last(5)

    def down_part(p):
        at = d_block(p)
        dg[:, at] = jnp.dot(h_t[...], tok[1, :, at], preferred_element_type=F32).astype(BF16)

    for p in near_first:
        with SC("downpart"): down_part(p)
        send(dg.at[:, d_block(p)], rd_ref.at[up_cols(z), :], dev(zz=p), "rd", "rd")
    with SC("downpartz"):
        down_part(z)
        rd_ref[up_cols(z), :] = dg[:, d_block(z)]

    with SC("wdwait"): arrived(wd.at[:, pl.ds(0, others)], "wd")

    def r0_rows(j, ff=None, n=0):
        if ff is None:
            return pl.ds(j * half, half)
        return pl.ds(pl.multiple_of(j * half + ff * pr + n * sub, sub), sub)

    def added(*terms):
        total = terms[0].astype(F32)
        for term in terms[1:]:
            total = total + term.astype(F32)
        return total.astype(BF16)

    def core_sum(j):
        p = blocks[j]
        arrived(r0.at[r0_rows(j), :], ("r0", j))
        for n in range(SUBS):
            for k, ff in ((1, f3), (0, f1)):
                at = sub_rows(p, ff, n)
                part[at, :] = added(part[at, :], r0[r0_rows(j, ff, n), :])
                key = ("r1", j, n) if k else ("r2", j, n)
                send(part.at[at, :], r1.at[j, k, n], dev(ff=f1), "late", key)
        for ff in (f2, f):
            at = rows(p, ff, c)
            part[at, :] = added(part[at, :], r0[pl.ds(pl.multiple_of(j * half + ff * pr, pr), pr), :])

    def part_rows(at):
        value = 2.0 * act[at, :] * contract_last(tok[1, at, :], wd[...])
        slopes[at, :] = value.astype(BF16)
        part[at, :] = contract_last(slopes[at, :], wu[...]).astype(BF16)

    def slopes_turned():
        @pl.loop(0, R * tl // step)
        def _(i):
            at = pl.ds(pl.multiple_of(i * step, step), step)
            s_t[:, at] = jnp.transpose(slopes[at, :].astype(F32)).astype(BF16)

    def first_sum(j, n):
        at = sub_rows(blocks[j], f2, n)
        arrived(r1.at[j, 1, n], ("r1", j, n))
        part[at, :] = added(part[at, :], r1[j, 1, n])
        send(part.at[at, :], r2.at[j, n], dev(ff=f2), "late", ("r2", j, n))

    def second_sum(j, n):
        at = sub_rows(blocks[j], f, n)
        arrived(part.at[pl.ds(0, 2 * sub), :], ("r2", j, n))
        part[at, :] = added(part[at, :], r1[j, 0, n], r2[j, n])

    R3 = dict(key="r3", count=(R + 1) * SUBS)

    def r3_at(p, side, n, ends):
        return jnp.where(jnp.logical_and(side == 1, ends), R, p) * SUBS + n

    def line_sum(j, n):
        p = blocks[j]
        at = sub_rows(p, f, n)
        side = jnp.where(p > z, 0, 1)

        @pl.when(beyond(p))
        def _():
            arrived(r3.at[p, side, n], index=p * SUBS + n, **R3)
            part[at, :] = added(part[at, :], r3[p, side, n])

        send(part.at[at, :], r3.at[p, side, n], dev(zz=toward(p)), "late", index=r3_at(p, side, n, p == toward(p)), **R3)

    def own_sum(n):
        at = sub_rows(z, f, n)
        for side, there in ((0, z > 0), (1, z < R - 1)):
            @pl.when(there)
            def _(side=side):
                arrived(r3.at[z, side, n], index=(R if side else z) * SUBS + n, **R3)
                part[at, :] = added(part[at, :], r3[z, side, n])
        ig_ref[piece_sub(f, c, n), :] = part[at, :]

    def piece_sub(ff, cc, n):
        return pl.ds(pl.multiple_of((cc * 4 + ff) * pr + n * sub, sub), sub)

    def up_part(p):
        at = d_block(p)
        ug[at, :] = jnp.transpose(jnp.dot(s_t[...], tok[0, :, at], preferred_element_type=F32)).astype(BF16)

    def send_up_part(p):
        send(ug.at[d_block(p), :], ru_ref.at[:, up_cols(z)], dev(zz=p), "ru", "ru")

    def fs(j, n):
        with SC(f"fs{j}{n}"): first_sum(j, n)

    def ss(j, n):
        with SC(f"ss{j}{n}"): second_sum(j, n)
        if j < R - 1:
            @pl.when(outer)
            def _():
                with SC(f"lsO{j}{n}"): line_sum(j, n)

    def ls(j, n):
        @pl.when(inner)
        def _():
            with SC(f"lsI{j}{n}"): line_sum(j, n)

    def turn(slot):
        with SC("uppart"): up_part(far_first[slot])

    for j, p in enumerate(blocks):
        theirs = core_rows(p, 1 - c)
        with SC(f"slopesA{j}"): part_rows(theirs)
        send(part.at[theirs, :], r0.at[r0_rows(j), :], dev(cc=1 - c), "late", ("r0", j))
        if j:
            with SC(f"core{j-1}"): core_sum(j - 1)
        if j == R - 1:
            fs(0, 0)
        with SC(f"slopesB{j}"): part_rows(core_rows(p, c))
    with SC(f"core{R-1}"): core_sum(R - 1)

    fs(0, 1)
    with SC("s_t"): slopes_turned()
    turn(0)
    pl.when(outer)(functools.partial(send_up_part, far_first[0]))
    ss(0, 0)
    fs(1, 0)
    turn(1)
    ss(0, 1)
    fs(1, 1)
    turn(2)
    pl.when(inner)(functools.partial(send_up_part, far_first[2]))
    ss(1, 0)
    with SC("uppartz"):
        up_part(z)
        ru_ref[:, up_cols(z)] = ug[d_block(z), :]
    fs(2, 0)
    ss(1, 1)
    ls(0, 0)
    fs(2, 1)
    ss(2, 0)
    ls(0, 1)
    fs(3, 0)
    ls(1, 0)
    ss(2, 1)

    @pl.when(outer)
    def _():
        send_up_part(far_first[1])
        send_up_part(far_first[2])

    ls(1, 1)

    @pl.when(inner)
    def _():
        send_up_part(far_first[0])
        send_up_part(far_first[1])

    fs(3, 1)
    ss(3, 0)
    ls(2, 0)
    ls(2, 1)

    with SC("earlysent"):
        sent(tok.at[:, pl.ds(0, (7 * R - 5) * pr), :], "early")
        pl.when(inner)(lambda: sent(part.at[pl.ds(0, 4 * pr), :], "fwd"))
        sent(wu.at[pl.ds(0, others), :], "wu")
        sent(wd.at[:, pl.ds(0, others)], "wd")
        sent(dg.at[:, pl.ds(0, others)], "rd")
    with SC("rdwait"):
        arrived(rd_ref.at[pl.ds(0, (R - 1) * h), :], "rd")
        down_ref[...] = rd_ref[...].astype(F32)

    size = pr // PIECES

    def gathered(n):
        def at(ff, cc):
            return ig_ref.at[pl.ds(pl.multiple_of((cc * 4 + ff) * pr + n * size, size), size), :]
        return spread(at, ("tok", n), "late")

    gather = [gathered(n) for n in range(PIECES)]
    with SC("own0"): own_sum(0)
    for n in range(PIECES // 2):
        gather[n][0]()
    ss(3, 1)
    with SC("own1"): own_sum(1)
    for n in range(PIECES // 2, PIECES):
        gather[n][0]()
    for n in range(PIECES // 2):
        with SC(f"ig1.{n}"): gather[n][1]()
    for n in range(PIECES // 2):
        with SC(f"ig1.{n+2}"): gather[n + PIECES // 2][1]()
        with SC(f"ig2.{n}"): gather[n][2]()
    for n in range(PIECES // 2, PIECES):
        with SC(f"ig2.{n}"): gather[n][2]()
    with SC("iglast"):
        for n in range(PIECES):
            arrived(ig_ref.at[pl.ds(0, 4 * size), :], ("tok", n, 4))

    with SC("ruwait"): arrived(ru_ref.at[:, pl.ds(0, (R - 1) * h)], "ru")

    with SC("sendwait"):
        sent(ug.at[pl.ds(0, others), :], "ru")
        sent(tok.at[:, pl.ds(0, (4 * R + 3) * pr), :], "late")
    for names, sems in ((send_names, send_sems), (recv_names, recv_sems)):
        assert sum(n for _, n in names.values()) == sems.shape[0], (names, sems.shape)


def in_planes(R, hidden_in, cotangent, w_up, w_down):
    tl, D = hidden_in.shape
    dl, fl = w_up.shape
    T, h, pr = tl * R, fl // R, tl // 8
    send_sems, recv_sems = 7, 11 * R - 4 + (3 * R + 1) * SUBS
    vmem = pl.BlockSpec(memory_space=pltpu.VMEM)
    input_grad, up, down = pl.pallas_call(
        functools.partial(kernel, R),
        out_shape=(
            pltpu.VMEM((tl, D), BF16),
            pltpu.VMEM((dl, fl), BF16),
            pltpu.VMEM((fl, dl), F32),
        ),
        in_specs=[pl.BlockSpec(memory_space=pl.ANY)] * 4,
        out_specs=(vmem, vmem, vmem),
        scratch_shapes=[
            pltpu.VMEM((fl, dl), BF16),
            pltpu.VMEM((2, pr, D), BF16),
            pltpu.VMEM((2, T, D), BF16),
            pltpu.VMEM((D, h), BF16),
            pltpu.VMEM((h, D), BF16),
            pltpu.VMEM((T, h), F32),
            pltpu.VMEM((T, h), BF16),
            pltpu.VMEM((h, T), BF16),
            pltpu.VMEM((h, T), BF16),
            pltpu.VMEM((T, D), BF16),
            pltpu.VMEM((R * 4 * pr, D), BF16),
            pltpu.VMEM((R, 2, SUBS, pr // SUBS, D), BF16),
            pltpu.VMEM((R, SUBS, pr // SUBS, D), BF16),
            pltpu.VMEM((R, 2, SUBS, pr // SUBS, D), BF16),
            pltpu.VMEM((D, h), BF16),
            pltpu.VMEM((h, D), BF16),
            pltpu.SemaphoreType.DMA((send_sems,)),
            pltpu.SemaphoreType.DMA((recv_sems,)),
            pltpu.SemaphoreType.DMA((5,)),
        ],
        compiler_params=pltpu.CompilerParams(
            collective_id=0, has_side_effects=True, vmem_limit_bytes=58 * 1024 * 1024
        ),
    )(hidden_in, cotangent, w_up, w_down)
    return written_out(input_grad, up, down)


def write_out(ig_ref, up_ref, down_ref, ig_out, up_out, down_out, wide, sems):
    copies = []
    for ref, out in ((down_ref, down_out), (ig_ref, ig_out)):
        n = ref.shape[0] // PARTS
        for i in range(PARTS):
            at = pl.ds(i * n, n)
            copies.append(pltpu.make_async_copy(ref.at[at, :], out.at[at, :], sems.at[len(copies)]))
            copies[-1].start()
    n = up_ref.shape[0] // CHUNKS
    for i in range(CHUNKS):
        at = pl.ds(i * n, n)
        wide[at, :] = up_ref[at, :].astype(F32)
        copies.append(pltpu.make_async_copy(wide.at[at, :], up_out.at[at, :], sems.at[len(copies)]))
        copies[-1].start()
    for copy in copies:
        copy.wait()


def written_out(input_grad, up, down):
    vmem = pl.BlockSpec(memory_space=pltpu.VMEM)
    there = [pltpu.with_memory_space_constraint(x, pltpu.VMEM) for x in (input_grad, up, down)]
    return pl.pallas_call(
        write_out,
        out_shape=(
            jax.ShapeDtypeStruct(input_grad.shape, BF16),
            jax.ShapeDtypeStruct(up.shape, F32),
            jax.ShapeDtypeStruct(down.shape, F32),
        ),
        in_specs=[vmem] * 3,
        out_specs=[pl.BlockSpec(memory_space=pl.ANY)] * 3,
        scratch_shapes=[pltpu.VMEM(up.shape, F32), pltpu.SemaphoreType.DMA((2 * PARTS + CHUNKS,))],
        compiler_params=pltpu.CompilerParams(vmem_limit_bytes=8 * 1024 * 1024),
    )(*there)


def solution(mesh):
    R, F, C = (mesh.shape[name] for name in ("rep", "fs", "tp"))
    body = functools.partial(in_planes, R) if (R, F, C) == (4, 4, 2) else plain
    return jax.shard_map(
        body,
        mesh=mesh,
        in_specs=(P("rep", None), P("rep", None), P("rep", ("fs", "tp")), P(("fs", "tp"), "rep")),
        out_specs=(P("rep", None), P("rep", ("fs", "tp")), P(("fs", "tp"), "rep")),
        check_vma=False,
    )
```

```python
import functools

import jax
import jax.numpy as jnp
from jax import lax
from jax.experimental import pallas as pl
from jax.experimental.pallas import tpu as pltpu
from jax.sharding import PartitionSpec as P

MESH = pl.DeviceIdType.MESH
BF16, F32 = jnp.bfloat16, jnp.float32


def contract_last(left, right):
    return lax.dot_general(left, right, (((1,), (1,)), ((), ())), preferred_element_type=F32)


def contract_first(left, right):
    return lax.dot_general(left, right, (((0,), (0,)), ((), ())), preferred_element_type=F32)


def plain(hidden_in, cotangent, w_up, w_down):
    up_full = lax.all_gather(w_up, "rep", axis=0, tiled=True)
    back_grad = contract_last(cotangent, lax.all_gather(w_down, "rep", axis=1, tiled=True))
    preact = jnp.dot(hidden_in, up_full, preferred_element_type=F32)
    active = jnp.maximum(preact, 0.0)
    hidden = (active * active).astype(BF16)
    slopes = (2.0 * active * back_grad).astype(BF16)
    grad_upper = lax.psum_scatter(
        contract_first(hidden_in, slopes).astype(BF16), "rep", scatter_dimension=0, tiled=True
    ).astype(F32)
    lower_rows = lax.psum_scatter(
        contract_first(cotangent, hidden).astype(BF16), "rep", scatter_dimension=0, tiled=True
    ).astype(F32)
    partial_sum = contract_last(slopes, up_full).astype(BF16)
    input_grad = lax.psum(partial_sum, ("fs", "tp")).astype(F32).astype(BF16)
    return (input_grad, grad_upper, lower_rows.T)


SC = jax.named_scope
SUBS, PIECES, CHUNKS = 2, 4, 4

def kernel(
    R, x_ref, g_ref, wu_in, wd_in,
    ig_ref, ru_ref, down_ref,
    rd_ref, stage, tok, wu, wd, act, slopes, s_t, h_t, part, r0, r1, r2, r3, ug, dg,
    send_sems, recv_sems, local_sems,
):
    z, f, c = lax.axis_index("rep"), lax.axis_index("fs"), lax.axis_index("tp")
    tl, D = x_ref.shape
    dl, fl = wu_in.shape
    h = fl // R
    pr = tl // 8
    half = 4 * pr
    sub = pr // SUBS
    steps = 2 * (R - 1)
    xx, yy = lax.rem(f, 2), lax.div(f, 2)
    fx, fy = yy * 2 + (1 - xx), (1 - yy) * 2 + xx
    f1 = fx * (1 - c) + fy * c
    f2 = fy * (1 - c) + fx * c
    f3 = 3 - f

    edge = jnp.minimum(z, R - 1 - z)
    far = jnp.where(z < R - 1 - z, 1, -1)
    inner = edge > 0
    outer = edge == 0

    def plane_at(slot):
        both = z + (slot // 2 + 1) * (2 * (slot % 2) - 1) * far
        return jnp.where(slot < 2 * edge, both, z + far * (slot + 1 - edge))

    near_first = [plane_at(slot) for slot in range(R - 1)]
    far_first = near_first[::-1]
    blocks = far_first + [z]

    def beyond(p):
        return jnp.logical_or(jnp.logical_and(p < z, z < R - 1), jnp.logical_and(p > z, z > 0))

    def past(p):
        return jnp.where(p < z, z + 1, z - 1)

    def toward(p):
        return jnp.where(p > z, z + 1, z - 1)

    send_names, recv_names = {}, {}

    def named(names, key, count):
        if key not in names:
            names[key] = sum(n for _, n in names.values()), count
        return names[key][0]

    def dev(zz=None, ff=None, cc=None):
        return {"rep": z if zz is None else zz, "fs": f if ff is None else ff, "tp": c if cc is None else cc}

    def remote(src, dst, device, group, key, index=0, count=1):
        return pltpu.make_async_remote_copy(
            src_ref=src, dst_ref=dst, send_sem=send_sems.at[named(send_names, group, 1)],
            recv_sem=recv_sems.at[named(recv_names, key, count) + index],
            device_id=device, device_id_type=MESH)

    def send(*args, **kw):
        remote(*args, **kw).start()

    def arrived(dst, key, index=0, count=1):
        pltpu.make_async_remote_copy(
            src_ref=dst, dst_ref=dst, send_sem=send_sems.at[0],
            recv_sem=recv_sems.at[named(recv_names, key, count) + index],
            device_id=dev(cc=1 - c), device_id_type=MESH).wait_recv()

    def sent(src, group):
        pltpu.make_async_remote_copy(
            src_ref=src, dst_ref=src, send_sem=send_sems.at[named(send_names, group, 1)],
            recv_sem=recv_sems.at[0], device_id=dev(cc=1 - c), device_id_type=MESH).wait_send()

    def sub_rows(zz, ff, n):
        return pl.ds(pl.multiple_of(zz * tl + (c * 4 + ff) * pr + n * sub, sub), sub)

    def rows(zz, ff, cc):
        return pl.ds(pl.multiple_of(zz * tl + (cc * 4 + ff) * pr, pr), pr)

    def core_rows(zz, cc):
        return pl.ds(pl.multiple_of(zz * tl + cc * half, half), half)

    def piece_rows(ff, cc):
        return pl.ds(pl.multiple_of((cc * 4 + ff) * pr, pr), pr)

    def up_cols(zz):
        return pl.ds(pl.multiple_of(zz * h, h), h)

    def d_block(zz):
        return pl.ds(pl.multiple_of(zz * dl, dl), dl)

    sources = (x_ref, g_ref)
    staged = [
        pltpu.make_async_copy(sources[a].at[piece_rows(f, c), :], stage.at[a], local_sems.at[a])
        for a in (0, 1)
    ]
    for copy in staged:
        copy.start()

    with SC("barrier"):
        barrier = pltpu.get_barrier_semaphore()
        near = [dev(zz=lax.rem(z + d, R)) for d in range(1, R)] + [dev(ff=fx), dev(ff=fy), dev(cc=1 - c)]
        for device in near:
            pl.semaphore_signal(barrier, inc=1, device_id=device, device_id_type=MESH)
        pl.semaphore_wait(barrier, len(near))

    TOK = dict(key="tok", count=2 * R)

    def send_own(a, to):
        send(stage.at[a], tok.at[a, rows(z, f, c), :], dev(zz=to), "early", index=a * R + z, **TOK)

    def send_up(p):
        send(wu_in.at[:, up_cols(p)], wu.at[d_block(z), :], dev(zz=p), "wu", "wu")

    def send_down(p):
        send(wd_in.at[up_cols(p), :], wd.at[:, d_block(z)], dev(zz=p), "wd", "wd")

    for a in (0, 1):
        staged[a].wait()
        send_own(a, near_first[0])
        send_own(a, near_first[1])

    @pl.when(outer)
    def _():
        send_up(near_first[0])
        send_up(near_first[1])
        send_down(near_first[1])
        send_down(near_first[0])
        send_up(near_first[2])

    @pl.when(inner)
    def _():
        for p in near_first[1:]:
            send_up(p)
        for p in near_first[1:]:
            send_down(p)

    own_rows = pl.ds(pl.multiple_of(z * tl, tl), tl)
    local = [
        pltpu.make_async_copy(x_ref, tok.at[0, own_rows, :], local_sems.at[2]),
        pltpu.make_async_copy(g_ref, tok.at[1, own_rows, :], local_sems.at[2]),
        pltpu.make_async_copy(wu_in.at[:, up_cols(z)], wu.at[d_block(z), :], local_sems.at[3]),
        pltpu.make_async_copy(wd_in.at[up_cols(z), :], wd.at[:, d_block(z)], local_sems.at[4]),
    ]
    for copy in local:
        copy.start()

    inner_order = [(0, 0), (0, 1), (0, 2), (1, 0), (1, 1), (1, 2)]
    outer_order = [(0, 0), (1, 0), (0, 1), (0, 2), (1, 1), (1, 2)]
    order = []
    for (ai, si), (ao, so) in zip(inner_order, outer_order):
        a = ai if ai == ao else jnp.where(inner, ai, ao)
        p = near_first[si] if si == so else jnp.where(inner, near_first[si], near_first[so])
        order.append((a, p))

    def spread(at, size, i, group):
        tag, whole = ("tok", i), ("whole", i // 4)

        def first():
            mine = at(f, c)
            send(mine, mine, dev(ff=f1), group, tag + (1,))
            send(mine, mine, dev(ff=f2), group, tag + (1,))
            send(mine, mine, dev(cc=1 - c), group, whole)

        def second():
            p1, p2 = at(f1, c), at(f2, c)
            arrived(part.at[pl.ds(0, 2 * size), :], tag + (1,))
            send(p1, p1, dev(ff=f2), group, tag + (3,))
            send(p1, p1, dev(cc=1 - c), group, whole)
            send(p2, p2, dev(cc=1 - c), group, whole)

        def third():
            p3 = at(f3, c)
            arrived(p3, tag + (3,))
            send(p3, p3, dev(cc=1 - c), group, whole)

        return first, second, third

    spreads = [
        spread(lambda ff, cc, a=a, p=p: tok.at[a, rows(p, ff, cc), :], pr, i, "early")
        for i, (a, p) in enumerate(order)
    ]

    def forward(i):
        a, p = order[i]
        mine = tok.at[a, rows(p, f, c), :]
        return remote(mine, mine, dev(zz=near_first[0]), "fwd", index=a * R + p, **TOK)

    def take(i):
        a, p = order[i]
        arrived(tok.at[a, rows(p, f, c), :], index=a * R + p, **TOK)
        pl.when(jnp.logical_and(inner, p != near_first[0]))(forward(i).start)

    def first(i):
        with SC(f"first{i}"): spreads[i][0]()

    def second(i):
        with SC(f"second{i}"): spreads[i][1]()

    def third(i):
        with SC(f"third{i}"): spreads[i][2]()

    def last(k):
        pieces = min(4, steps - 4 * k)
        with SC(f"last{k}"): arrived(tok.at[0, pl.ds(0, pieces * half), :], ("whole", k))

    def take_in(*which):
        @pl.when(inner)
        def _():
            for i in which:
                if i < steps:
                    with SC(f"takeI{i}"): take(i)

    def take_out(*which):
        @pl.when(outer)
        def _():
            for i in which:
                if i < steps:
                    with SC(f"takeO{i}"): take(i)

    take_in(0)
    take_out(0)
    first(0)
    take_in(1)
    take_out(1)
    first(1)
    take_in(2)
    second(0)
    take_out(2)
    first(2)
    take_in(3, 4)
    second(1)
    third(0)
    take_out(3)
    first(3)
    take_in(5)


    @pl.when(inner)
    def _():
        send_up(near_first[0])
        send_down(near_first[0])

    second(2)
    third(1)
    take_out(4)
    first(4)
    second(3)
    third(2)
    take_out(5)
    pl.when(outer)(functools.partial(send_down, near_first[2]))
    first(5)
    second(4)
    third(3)
    second(5)
    third(4)

    step = min(tl, 256)

    def up_block(p):
        @pl.loop(0, tl // step)
        def _(i):
            at = pl.ds(pl.multiple_of(p * tl + i * step, step), step)
            active = jnp.maximum(jnp.dot(tok[0, at, :], wu[...], preferred_element_type=F32), 0.0)
            act[at, :] = active
            h_t[:, at] = jnp.transpose(active * active).astype(BF16)

    own_tokens = tok.at[:, own_rows, :]
    pltpu.make_async_copy(own_tokens, own_tokens, local_sems.at[2]).wait()
    for copy in local[2:]:
        copy.wait()
    others = (R - 1) * dl
    with SC("wuwait"): arrived(wu.at[pl.ds(0, others), :], "wu")
    with SC("upz"): up_block(z)
    last(0)
    for slot in range(R - 1):
        with SC(f"up{slot}"): up_block(near_first[slot])
    third(5)
    last(1)

    def down_part(p):
        at = d_block(p)
        dg[:, at] = jnp.dot(h_t[...], tok[1, :, at], preferred_element_type=F32).astype(BF16)

    for p in near_first:
        with SC("downpart"): down_part(p)
        send(dg.at[:, d_block(p)], rd_ref.at[up_cols(z), :], dev(zz=p), "rd", "rd")
    with SC("downpartz"):
        down_part(z)
        rd_ref[up_cols(z), :] = dg[:, d_block(z)]

    with SC("wdwait"): arrived(wd.at[:, pl.ds(0, others)], "wd")

    def r0_rows(j, ff=None, n=0):
        if ff is None:
            return pl.ds(j * half, half)
        return pl.ds(pl.multiple_of(j * half + ff * pr + n * sub, sub), sub)

    def added(*terms):
        total = terms[0].astype(F32)
        for term in terms[1:]:
            total = total + term.astype(F32)
        return total.astype(BF16)

    def core_sum(j):
        p = blocks[j]
        arrived(r0.at[r0_rows(j), :], ("r0", j))
        for n in range(SUBS):
            for k, ff in ((1, f3), (0, f1)):
                at = sub_rows(p, ff, n)
                part[at, :] = added(part[at, :], r0[r0_rows(j, ff, n), :])
                key = ("r1", j, n) if k else ("r2", j, n)
                send(part.at[at, :], r1.at[j, k, n], dev(ff=f1), "late", key)
        for ff in (f2, f):
            at = rows(p, ff, c)
            part[at, :] = added(part[at, :], r0[pl.ds(pl.multiple_of(j * half + ff * pr, pr), pr), :])

    def part_rows(at):
        value = 2.0 * act[at, :] * contract_last(tok[1, at, :], wd[...])
        slopes[at, :] = value.astype(BF16)
        part[at, :] = contract_last(slopes[at, :], wu[...]).astype(BF16)

    def slopes_turned():
        @pl.loop(0, R * tl // step)
        def _(i):
            at = pl.ds(pl.multiple_of(i * step, step), step)
            s_t[:, at] = jnp.transpose(slopes[at, :].astype(F32)).astype(BF16)

    def first_sum(j, n):
        at = sub_rows(blocks[j], f2, n)
        arrived(r1.at[j, 1, n], ("r1", j, n))
        part[at, :] = added(part[at, :], r1[j, 1, n])
        send(part.at[at, :], r2.at[j, n], dev(ff=f2), "late", ("r2", j, n))

    def second_sum(j, n):
        at = sub_rows(blocks[j], f, n)
        arrived(part.at[pl.ds(0, 2 * sub), :], ("r2", j, n))
        part[at, :] = added(part[at, :], r1[j, 0, n], r2[j, n])

    R3 = dict(key="r3", count=(R + 1) * SUBS)

    def r3_at(p, side, n, ends):
        return jnp.where(jnp.logical_and(side == 1, ends), R, p) * SUBS + n

    def line_sum(j, n):
        p = blocks[j]
        at = sub_rows(p, f, n)
        side = jnp.where(p > z, 0, 1)

        @pl.when(beyond(p))
        def _():
            arrived(r3.at[p, side, n], index=p * SUBS + n, **R3)
            part[at, :] = added(part[at, :], r3[p, side, n])

        send(part.at[at, :], r3.at[p, side, n], dev(zz=toward(p)), "late", index=r3_at(p, side, n, p == toward(p)), **R3)

    def own_sum(n):
        at = sub_rows(z, f, n)
        for side, there in ((0, z > 0), (1, z < R - 1)):
            @pl.when(there)
            def _(side=side):
                arrived(r3.at[z, side, n], index=(R if side else z) * SUBS + n, **R3)
                part[at, :] = added(part[at, :], r3[z, side, n])
        ig_ref[piece_sub(f, c, n), :] = part[at, :]

    def piece_sub(ff, cc, n):
        return pl.ds(pl.multiple_of((cc * 4 + ff) * pr + n * sub, sub), sub)

    def up_part(p):
        at = d_block(p)
        ug[at, :] = jnp.transpose(jnp.dot(s_t[...], tok[0, :, at], preferred_element_type=F32)).astype(BF16)

    def send_up_part(p):
        send(ug.at[d_block(p), :], ru_ref.at[:, up_cols(z)], dev(zz=p), "ru", "ru")

    def fs(j, n):
        with SC(f"fs{j}{n}"): first_sum(j, n)

    def ss(j, n):
        with SC(f"ss{j}{n}"): second_sum(j, n)
        if j < R - 1:
            @pl.when(outer)
            def _():
                with SC(f"lsO{j}{n}"): line_sum(j, n)

    def ls(j, n):
        @pl.when(inner)
        def _():
            with SC(f"lsI{j}{n}"): line_sum(j, n)

    def turn(slot):
        with SC("uppart"): up_part(far_first[slot])

    for j, p in enumerate(blocks):
        theirs = core_rows(p, 1 - c)
        with SC(f"slopesA{j}"): part_rows(theirs)
        send(part.at[theirs, :], r0.at[r0_rows(j), :], dev(cc=1 - c), "late", ("r0", j))
        if j:
            with SC(f"core{j-1}"): core_sum(j - 1)
        if j == R - 1:
            fs(0, 0)
        with SC(f"slopesB{j}"): part_rows(core_rows(p, c))
    with SC(f"core{R-1}"): core_sum(R - 1)

    fs(0, 1)
    with SC("s_t"): slopes_turned()
    turn(0)
    pl.when(outer)(functools.partial(send_up_part, far_first[0]))
    ss(0, 0)
    fs(1, 0)
    turn(1)
    ss(0, 1)
    fs(1, 1)
    turn(2)
    pl.when(inner)(functools.partial(send_up_part, far_first[2]))
    ss(1, 0)
    with SC("uppartz"):
        up_part(z)
        ru_ref[:, up_cols(z)] = ug[d_block(z), :]
    fs(2, 0)
    ss(1, 1)
    ls(0, 0)
    fs(2, 1)
    ss(2, 0)
    ls(0, 1)
    fs(3, 0)
    ls(1, 0)
    ss(2, 1)

    @pl.when(outer)
    def _():
        send_up_part(far_first[1])
        send_up_part(far_first[2])

    ls(1, 1)

    @pl.when(inner)
    def _():
        send_up_part(far_first[0])
        send_up_part(far_first[1])

    fs(3, 1)
    ss(3, 0)
    ls(2, 0)
    ls(2, 1)

    with SC("earlysent"):
        sent(tok.at[:, pl.ds(0, (7 * R - 5) * pr), :], "early")
        pl.when(inner)(lambda: sent(part.at[pl.ds(0, 4 * pr), :], "fwd"))
        sent(wu.at[pl.ds(0, others), :], "wu")
        sent(wd.at[:, pl.ds(0, others)], "wd")
        sent(dg.at[:, pl.ds(0, others)], "rd")
    with SC("rdwait"):
        arrived(rd_ref.at[pl.ds(0, (R - 1) * h), :], "rd")
        down_ref[...] = rd_ref[...].astype(F32)

    size = pr // PIECES

    def gathered(n):
        def at(ff, cc):
            return ig_ref.at[pl.ds(pl.multiple_of((cc * 4 + ff) * pr + n * size, size), size), :]
        return spread(at, size, n, "late")

    gather = [gathered(n) for n in range(PIECES)]
    with SC("own0"): own_sum(0)
    for n in range(PIECES // 2):
        gather[n][0]()
    ss(3, 1)
    with SC("own1"): own_sum(1)
    for n in range(PIECES // 2, PIECES):
        gather[n][0]()
    for n in range(PIECES // 2):
        with SC(f"ig1.{n}"): gather[n][1]()
    for n in range(PIECES // 2):
        with SC(f"ig1.{n+2}"): gather[n + PIECES // 2][1]()
        with SC(f"ig2.{n}"): gather[n][2]()
    for n in range(PIECES // 2, PIECES):
        with SC(f"ig2.{n}"): gather[n][2]()
    with SC("iglast"):
        arrived(ig_ref.at[pl.ds(0, half), :], ("whole", 0))

    with SC("ruwait"): arrived(ru_ref.at[:, pl.ds(0, (R - 1) * h)], "ru")

    with SC("sendwait"):
        sent(ug.at[pl.ds(0, others), :], "ru")
        sent(tok.at[:, pl.ds(0, (4 * R + 3) * pr), :], "late")
    for names, sems in ((send_names, send_sems), (recv_names, recv_sems)):
        assert sum(n for _, n in names.values()) == sems.shape[0], (names, sems.shape)


def in_planes(R, hidden_in, cotangent, w_up, w_down):
    tl, D = hidden_in.shape
    dl, fl = w_up.shape
    T, h, pr = tl * R, fl // R, tl // 8
    send_sems, recv_sems = 7, 7 * R + 2 + (3 * R + 1) * SUBS
    vmem = pl.BlockSpec(memory_space=pltpu.VMEM)
    input_grad, up, down = pl.pallas_call(
        functools.partial(kernel, R),
        out_shape=(
            pltpu.VMEM((tl, D), BF16),
            pltpu.VMEM((dl, fl), BF16),
            pltpu.VMEM((fl, dl), F32),
        ),
        in_specs=[pl.BlockSpec(memory_space=pl.ANY)] * 4,
        out_specs=(vmem, vmem, vmem),
        scratch_shapes=[
            pltpu.VMEM((fl, dl), BF16),
            pltpu.VMEM((2, pr, D), BF16),
            pltpu.VMEM((2, T, D), BF16),
            pltpu.VMEM((D, h), BF16),
            pltpu.VMEM((h, D), BF16),
            pltpu.VMEM((T, h), F32),
            pltpu.VMEM((T, h), BF16),
            pltpu.VMEM((h, T), BF16),
            pltpu.VMEM((h, T), BF16),
            pltpu.VMEM((T, D), BF16),
            pltpu.VMEM((R * 4 * pr, D), BF16),
            pltpu.VMEM((R, 2, SUBS, pr // SUBS, D), BF16),
            pltpu.VMEM((R, SUBS, pr // SUBS, D), BF16),
            pltpu.VMEM((R, 2, SUBS, pr // SUBS, D), BF16),
            pltpu.VMEM((D, h), BF16),
            pltpu.VMEM((h, D), BF16),
            pltpu.SemaphoreType.DMA((send_sems,)),
            pltpu.SemaphoreType.DMA((recv_sems,)),
            pltpu.SemaphoreType.DMA((5,)),
        ],
        compiler_params=pltpu.CompilerParams(
            collective_id=0, has_side_effects=True, vmem_limit_bytes=58 * 1024 * 1024
        ),
    )(hidden_in, cotangent, w_up, w_down)
    return written_out(input_grad, up, down)


def write_out(ig_ref, up_ref, down_ref, ig_out, up_out, down_out, wide, sems):
    whole = [
        pltpu.make_async_copy(down_ref, down_out, sems.at[0]),
        pltpu.make_async_copy(ig_ref, ig_out, sems.at[1]),
    ]
    for copy in whole:
        copy.start()
    n = up_ref.shape[0] // CHUNKS
    for i in range(CHUNKS):
        at = pl.ds(i * n, n)
        wide[at, :] = up_ref[at, :].astype(F32)
        pltpu.make_async_copy(wide.at[at, :], up_out.at[at, :], sems.at[2]).start()
    for copy in whole + [pltpu.make_async_copy(wide, up_out, sems.at[2])]:
        copy.wait()


def written_out(input_grad, up, down):
    vmem = pl.BlockSpec(memory_space=pltpu.VMEM)
    there = [pltpu.with_memory_space_constraint(x, pltpu.VMEM) for x in (input_grad, up, down)]
    return pl.pallas_call(
        write_out,
        out_shape=(
            jax.ShapeDtypeStruct(input_grad.shape, BF16),
            jax.ShapeDtypeStruct(up.shape, F32),
            jax.ShapeDtypeStruct(down.shape, F32),
        ),
        in_specs=[vmem] * 3,
        out_specs=[pl.BlockSpec(memory_space=pl.ANY)] * 3,
        scratch_shapes=[pltpu.VMEM(up.shape, F32), pltpu.SemaphoreType.DMA((3,))],
        compiler_params=pltpu.CompilerParams(vmem_limit_bytes=8 * 1024 * 1024),
    )(*there)


def solution(mesh):
    R, F, C = (mesh.shape[name] for name in ("rep", "fs", "tp"))
    body = functools.partial(in_planes, R) if (R, F, C) == (4, 4, 2) else plain
    return jax.shard_map(
        body,
        mesh=mesh,
        in_specs=(P("rep", None), P("rep", None), P("rep", ("fs", "tp")), P(("fs", "tp"), "rep")),
        out_specs=(P("rep", None), P("rep", ("fs", "tp")), P(("fs", "tp"), "rep")),
        check_vma=False,
    )
```

```python
import functools

import jax
import jax.numpy as jnp
from jax import lax
from jax.experimental import pallas as pl
from jax.experimental.pallas import tpu as pltpu
from jax.sharding import PartitionSpec as P

MESH = pl.DeviceIdType.MESH
BF16, F32 = jnp.bfloat16, jnp.float32


def contract_last(left, right):
    return lax.dot_general(left, right, (((1,), (1,)), ((), ())), preferred_element_type=F32)


def contract_first(left, right):
    return lax.dot_general(left, right, (((0,), (0,)), ((), ())), preferred_element_type=F32)


def plain(hidden_in, cotangent, w_up, w_down):
    up_full = lax.all_gather(w_up, "rep", axis=0, tiled=True)
    back_grad = contract_last(cotangent, lax.all_gather(w_down, "rep", axis=1, tiled=True))
    preact = jnp.dot(hidden_in, up_full, preferred_element_type=F32)
    active = jnp.maximum(preact, 0.0)
    hidden = (active * active).astype(BF16)
    slopes = (2.0 * active * back_grad).astype(BF16)
    grad_upper = lax.psum_scatter(
        contract_first(hidden_in, slopes).astype(BF16), "rep", scatter_dimension=0, tiled=True
    ).astype(F32)
    lower_rows = lax.psum_scatter(
        contract_first(cotangent, hidden).astype(BF16), "rep", scatter_dimension=0, tiled=True
    ).astype(F32)
    partial_sum = contract_last(slopes, up_full).astype(BF16)
    input_grad = lax.psum(partial_sum, ("fs", "tp")).astype(F32).astype(BF16)
    return (input_grad, grad_upper, lower_rows.T)


SC = jax.named_scope
SUBS, PIECES, CHUNKS = 2, 4, 4

def kernel(
    R, x_ref, g_ref, wu_in, wd_in,
    ig_ref, ru_ref, down_ref,
    rd_ref, stage, tok, wu, wd, act, slopes, s_t, h_t, part, r0, r1, r2, r3, ug, dg,
    send_sems, recv_sems, local_sems,
):
    z, f, c = lax.axis_index("rep"), lax.axis_index("fs"), lax.axis_index("tp")
    tl, D = x_ref.shape
    dl, fl = wu_in.shape
    h = fl // R
    pr = tl // 8
    half = 4 * pr
    sub = pr // SUBS
    steps = 2 * (R - 1)
    xx, yy = lax.rem(f, 2), lax.div(f, 2)
    fx, fy = yy * 2 + (1 - xx), (1 - yy) * 2 + xx
    f1 = fx * (1 - c) + fy * c
    f2 = fy * (1 - c) + fx * c
    f3 = 3 - f

    edge = jnp.minimum(z, R - 1 - z)
    far = jnp.where(z < R - 1 - z, 1, -1)
    inner = edge > 0
    outer = edge == 0

    def plane_at(slot):
        both = z + (slot // 2 + 1) * (2 * (slot % 2) - 1) * far
        return jnp.where(slot < 2 * edge, both, z + far * (slot + 1 - edge))

    near_first = [plane_at(slot) for slot in range(R - 1)]
    far_first = near_first[::-1]
    blocks = far_first + [z]

    def beyond(p):
        return jnp.logical_or(jnp.logical_and(p < z, z < R - 1), jnp.logical_and(p > z, z > 0))

    def past(p):
        return jnp.where(p < z, z + 1, z - 1)

    def toward(p):
        return jnp.where(p > z, z + 1, z - 1)

    send_names, recv_names = {}, {}

    def named(names, key, count):
        if key not in names:
            names[key] = sum(n for _, n in names.values()), count
        return names[key][0]

    def dev(zz=None, ff=None, cc=None):
        return {"rep": z if zz is None else zz, "fs": f if ff is None else ff, "tp": c if cc is None else cc}

    def remote(src, dst, device, group, key, index=0, count=1):
        return pltpu.make_async_remote_copy(
            src_ref=src, dst_ref=dst, send_sem=send_sems.at[named(send_names, group, 1)],
            recv_sem=recv_sems.at[named(recv_names, key, count) + index],
            device_id=device, device_id_type=MESH)

    def send(*args, **kw):
        remote(*args, **kw).start()

    def arrived(dst, key, index=0, count=1):
        pltpu.make_async_remote_copy(
            src_ref=dst, dst_ref=dst, send_sem=send_sems.at[0],
            recv_sem=recv_sems.at[named(recv_names, key, count) + index],
            device_id=dev(cc=1 - c), device_id_type=MESH).wait_recv()

    def sent(src, group):
        pltpu.make_async_remote_copy(
            src_ref=src, dst_ref=src, send_sem=send_sems.at[named(send_names, group, 1)],
            recv_sem=recv_sems.at[0], device_id=dev(cc=1 - c), device_id_type=MESH).wait_send()

    def sub_rows(zz, ff, n):
        return pl.ds(pl.multiple_of(zz * tl + (c * 4 + ff) * pr + n * sub, sub), sub)

    def rows(zz, ff, cc):
        return pl.ds(pl.multiple_of(zz * tl + (cc * 4 + ff) * pr, pr), pr)

    def core_rows(zz, cc):
        return pl.ds(pl.multiple_of(zz * tl + cc * half, half), half)

    def piece_rows(ff, cc):
        return pl.ds(pl.multiple_of((cc * 4 + ff) * pr, pr), pr)

    def up_cols(zz):
        return pl.ds(pl.multiple_of(zz * h, h), h)

    def d_block(zz):
        return pl.ds(pl.multiple_of(zz * dl, dl), dl)

    sources = (x_ref, g_ref)
    staged = [
        pltpu.make_async_copy(sources[a].at[piece_rows(f, c), :], stage.at[a], local_sems.at[a])
        for a in (0, 1)
    ]
    for copy in staged:
        copy.start()

    with SC("barrier"):
        barrier = pltpu.get_barrier_semaphore()
        near = [dev(zz=lax.rem(z + d, R)) for d in range(1, R)] + [dev(ff=fx), dev(ff=fy), dev(cc=1 - c)]
        for device in near:
            pl.semaphore_signal(barrier, inc=1, device_id=device, device_id_type=MESH)
        pl.semaphore_wait(barrier, len(near))

    TOK = dict(key="tok", count=2 * R)

    def send_own(a, to):
        send(stage.at[a], tok.at[a, rows(z, f, c), :], dev(zz=to), "early", index=a * R + z, **TOK)

    def send_up(p):
        send(wu_in.at[:, up_cols(p)], wu.at[d_block(z), :], dev(zz=p), "early", "wu")

    def send_down(p):
        send(wd_in.at[up_cols(p), :], wd.at[:, d_block(z)], dev(zz=p), "early", "wd")

    for a in (0, 1):
        staged[a].wait()
        send_own(a, near_first[0])
        send_own(a, near_first[1])

    @pl.when(outer)
    def _():
        send_up(near_first[0])
        send_up(near_first[1])
        send_down(near_first[1])
        send_down(near_first[0])
        send_up(near_first[2])

    @pl.when(inner)
    def _():
        for p in near_first[1:]:
            send_up(p)
        for p in near_first[1:]:
            send_down(p)

    own_rows = pl.ds(pl.multiple_of(z * tl, tl), tl)
    local = [
        pltpu.make_async_copy(x_ref, tok.at[0, own_rows, :], local_sems.at[2]),
        pltpu.make_async_copy(g_ref, tok.at[1, own_rows, :], local_sems.at[2]),
        pltpu.make_async_copy(wu_in.at[:, up_cols(z)], wu.at[d_block(z), :], local_sems.at[3]),
        pltpu.make_async_copy(wd_in.at[up_cols(z), :], wd.at[:, d_block(z)], local_sems.at[4]),
    ]
    for copy in local:
        copy.start()

    inner_order = [(0, 0), (0, 1), (0, 2), (1, 0), (1, 1), (1, 2)]
    outer_order = [(0, 0), (1, 0), (0, 1), (0, 2), (1, 1), (1, 2)]
    order = []
    for (ai, si), (ao, so) in zip(inner_order, outer_order):
        a = ai if ai == ao else jnp.where(inner, ai, ao)
        p = near_first[si] if si == so else jnp.where(inner, near_first[si], near_first[so])
        order.append((a, p))

    def spread(at, size, i, group):
        tag, whole = ("tok", i), ("whole", i // 4)

        def first():
            mine = at(f, c)
            send(mine, mine, dev(ff=f1), group, tag + (1,))
            send(mine, mine, dev(ff=f2), group, tag + (1,))
            send(mine, mine, dev(cc=1 - c), group, whole)

        def second():
            p1, p2 = at(f1, c), at(f2, c)
            arrived(part.at[pl.ds(0, 2 * size), :], tag + (1,))
            send(p1, p1, dev(ff=f2), group, tag + (3,))
            send(p1, p1, dev(cc=1 - c), group, whole)
            send(p2, p2, dev(cc=1 - c), group, whole)

        def third():
            p3 = at(f3, c)
            arrived(p3, tag + (3,))
            send(p3, p3, dev(cc=1 - c), group, whole)

        return first, second, third

    spreads = [
        spread(lambda ff, cc, a=a, p=p: tok.at[a, rows(p, ff, cc), :], pr, i, "early")
        for i, (a, p) in enumerate(order)
    ]

    def forward(i):
        a, p = order[i]
        mine = tok.at[a, rows(p, f, c), :]
        return remote(mine, mine, dev(zz=near_first[0]), "fwd", index=a * R + p, **TOK)

    def take(i):
        a, p = order[i]
        arrived(tok.at[a, rows(p, f, c), :], index=a * R + p, **TOK)
        pl.when(jnp.logical_and(inner, p != near_first[0]))(forward(i).start)

    def first(i):
        with SC(f"first{i}"): spreads[i][0]()

    def second(i):
        with SC(f"second{i}"): spreads[i][1]()

    def third(i):
        with SC(f"third{i}"): spreads[i][2]()

    def last(k):
        pieces = min(4, steps - 4 * k)
        with SC(f"last{k}"): arrived(tok.at[0, pl.ds(0, pieces * half), :], ("whole", k))

    def take_in(*which):
        @pl.when(inner)
        def _():
            for i in which:
                if i < steps:
                    with SC(f"takeI{i}"): take(i)

    def take_out(*which):
        @pl.when(outer)
        def _():
            for i in which:
                if i < steps:
                    with SC(f"takeO{i}"): take(i)

    take_in(0)
    take_out(0)
    first(0)
    take_in(1)
    take_out(1)
    first(1)
    take_in(2)
    second(0)
    take_out(2)
    first(2)
    take_in(3, 4)
    second(1)
    third(0)
    take_out(3)
    first(3)
    take_in(5)


    @pl.when(inner)
    def _():
        send_up(near_first[0])
        send_down(near_first[0])

    second(2)
    third(1)
    take_out(4)
    first(4)
    second(3)
    third(2)
    take_out(5)
    pl.when(outer)(functools.partial(send_down, near_first[2]))
    first(5)
    second(4)
    third(3)
    second(5)
    third(4)

    step = min(tl, 256)

    def up_block(p):
        @pl.loop(0, tl // step)
        def _(i):
            at = pl.ds(pl.multiple_of(p * tl + i * step, step), step)
            active = jnp.maximum(jnp.dot(tok[0, at, :], wu[...], preferred_element_type=F32), 0.0)
            act[at, :] = active
            h_t[:, at] = jnp.transpose(active * active).astype(BF16)

    own_tokens = tok.at[:, own_rows, :]
    pltpu.make_async_copy(own_tokens, own_tokens, local_sems.at[2]).wait()
    for copy in local[2:]:
        copy.wait()
    others = (R - 1) * dl
    with SC("wuwait"): arrived(wu.at[pl.ds(0, others), :], "wu")
    with SC("upz"): up_block(z)
    last(0)
    for slot in range(R - 1):
        with SC(f"up{slot}"): up_block(near_first[slot])
    third(5)
    last(1)

    def down_part(p):
        at = d_block(p)
        dg[:, at] = jnp.dot(h_t[...], tok[1, :, at], preferred_element_type=F32).astype(BF16)

    for p in near_first:
        with SC("downpart"): down_part(p)
        send(dg.at[:, d_block(p)], rd_ref.at[up_cols(z), :], dev(zz=p), "late", "rd")
    with SC("downpartz"):
        down_part(z)
        rd_ref[up_cols(z), :] = dg[:, d_block(z)]

    with SC("wdwait"): arrived(wd.at[:, pl.ds(0, others)], "wd")

    def r0_rows(j, ff=None, n=0):
        if ff is None:
            return pl.ds(j * half, half)
        return pl.ds(pl.multiple_of(j * half + ff * pr + n * sub, sub), sub)

    def added(*terms):
        total = terms[0].astype(F32)
        for term in terms[1:]:
            total = total + term.astype(F32)
        return total.astype(BF16)

    def core_sum(j):
        p = blocks[j]
        arrived(r0.at[r0_rows(j), :], ("r0", j))
        for n in range(SUBS):
            for k, ff in ((1, f3), (0, f1)):
                at = sub_rows(p, ff, n)
                part[at, :] = added(part[at, :], r0[r0_rows(j, ff, n), :])
                key = ("r1", j, n) if k else ("r2", j, n)
                send(part.at[at, :], r1.at[j, k, n], dev(ff=f1), "late", key)
        for ff in (f2, f):
            at = rows(p, ff, c)
            part[at, :] = added(part[at, :], r0[pl.ds(pl.multiple_of(j * half + ff * pr, pr), pr), :])

    def part_rows(at):
        value = 2.0 * act[at, :] * contract_last(tok[1, at, :], wd[...])
        slopes[at, :] = value.astype(BF16)
        part[at, :] = contract_last(slopes[at, :], wu[...]).astype(BF16)

    def slopes_turned():
        @pl.loop(0, R * tl // step)
        def _(i):
            at = pl.ds(pl.multiple_of(i * step, step), step)
            s_t[:, at] = jnp.transpose(slopes[at, :].astype(F32)).astype(BF16)

    def first_sum(j, n):
        at = sub_rows(blocks[j], f2, n)
        arrived(r1.at[j, 1, n], ("r1", j, n))
        part[at, :] = added(part[at, :], r1[j, 1, n])
        send(part.at[at, :], r2.at[j, n], dev(ff=f2), "late", ("r2", j, n))

    def second_sum(j, n):
        at = sub_rows(blocks[j], f, n)
        arrived(part.at[pl.ds(0, 2 * sub), :], ("r2", j, n))
        part[at, :] = added(part[at, :], r1[j, 0, n], r2[j, n])

    R3 = dict(key="r3", count=(R + 1) * SUBS)

    def r3_at(p, side, n, ends):
        return jnp.where(jnp.logical_and(side == 1, ends), R, p) * SUBS + n

    def line_sum(j, n):
        p = blocks[j]
        at = sub_rows(p, f, n)
        side = jnp.where(p > z, 0, 1)

        @pl.when(beyond(p))
        def _():
            arrived(r3.at[p, side, n], index=p * SUBS + n, **R3)
            part[at, :] = added(part[at, :], r3[p, side, n])

        send(part.at[at, :], r3.at[p, side, n], dev(zz=toward(p)), "late", index=r3_at(p, side, n, p == toward(p)), **R3)

    def own_sum(n):
        at = sub_rows(z, f, n)
        for side, there in ((0, z > 0), (1, z < R - 1)):
            @pl.when(there)
            def _(side=side):
                arrived(r3.at[z, side, n], index=(R if side else z) * SUBS + n, **R3)
                part[at, :] = added(part[at, :], r3[z, side, n])
        ig_ref[piece_sub(f, c, n), :] = part[at, :]

    def piece_sub(ff, cc, n):
        return pl.ds(pl.multiple_of((cc * 4 + ff) * pr + n * sub, sub), sub)

    def up_part(p):
        at = d_block(p)
        ug[at, :] = jnp.transpose(jnp.dot(s_t[...], tok[0, :, at], preferred_element_type=F32)).astype(BF16)

    def send_up_part(p):
        send(ug.at[d_block(p), :], ru_ref.at[:, up_cols(z)], dev(zz=p), "late", "ru")

    def fs(j, n):
        with SC(f"fs{j}{n}"): first_sum(j, n)

    def ss(j, n):
        with SC(f"ss{j}{n}"): second_sum(j, n)
        if j < R - 1:
            @pl.when(outer)
            def _():
                with SC(f"lsO{j}{n}"): line_sum(j, n)

    def ls(j, n):
        @pl.when(inner)
        def _():
            with SC(f"lsI{j}{n}"): line_sum(j, n)

    def turn(slot):
        with SC("uppart"): up_part(far_first[slot])

    for j, p in enumerate(blocks):
        theirs = core_rows(p, 1 - c)
        with SC(f"slopesA{j}"): part_rows(theirs)
        send(part.at[theirs, :], r0.at[r0_rows(j), :], dev(cc=1 - c), "late", ("r0", j))
        if j:
            with SC(f"core{j-1}"): core_sum(j - 1)
        if j == R - 1:
            fs(0, 0)
        with SC(f"slopesB{j}"): part_rows(core_rows(p, c))
    with SC(f"core{R-1}"): core_sum(R - 1)

    fs(0, 1)
    with SC("s_t"): slopes_turned()
    turn(0)
    pl.when(outer)(functools.partial(send_up_part, far_first[0]))
    ss(0, 0)
    fs(1, 0)
    turn(1)
    ss(0, 1)
    fs(1, 1)
    turn(2)
    pl.when(inner)(functools.partial(send_up_part, far_first[2]))
    ss(1, 0)
    with SC("uppartz"):
        up_part(z)
        ru_ref[:, up_cols(z)] = ug[d_block(z), :]
    fs(2, 0)
    ss(1, 1)
    ls(0, 0)
    fs(2, 1)
    ss(2, 0)
    ls(0, 1)
    fs(3, 0)
    ls(1, 0)
    ss(2, 1)

    @pl.when(outer)
    def _():
        send_up_part(far_first[1])
        send_up_part(far_first[2])

    ls(1, 1)

    @pl.when(inner)
    def _():
        send_up_part(far_first[0])
        send_up_part(far_first[1])

    fs(3, 1)
    ss(3, 0)
    ls(2, 0)
    ls(2, 1)

    with SC("earlysent"):
        sent(tok.at[:, pl.ds(0, (7 * R - 5) * pr + others * h // D), :], "early")
        pl.when(inner)(lambda: sent(part.at[pl.ds(0, 4 * pr), :], "fwd"))
    with SC("rdwait"):
        arrived(rd_ref.at[pl.ds(0, (R - 1) * h), :], "rd")
        down_ref[...] = rd_ref[...].astype(F32)

    size = pr // PIECES

    def gathered(n):
        def at(ff, cc):
            return ig_ref.at[pl.ds(pl.multiple_of((cc * 4 + ff) * pr + n * size, size), size), :]
        return spread(at, size, n, "late")

    gather = [gathered(n) for n in range(PIECES)]
    with SC("own0"): own_sum(0)
    for n in range(PIECES // 2):
        gather[n][0]()
    ss(3, 1)
    with SC("own1"): own_sum(1)
    for n in range(PIECES // 2, PIECES):
        gather[n][0]()
    for n in range(PIECES // 2):
        with SC(f"ig1.{n}"): gather[n][1]()
    for n in range(PIECES // 2):
        with SC(f"ig1.{n+2}"): gather[n + PIECES // 2][1]()
        with SC(f"ig2.{n}"): gather[n][2]()
    for n in range(PIECES // 2, PIECES):
        with SC(f"ig2.{n}"): gather[n][2]()
    with SC("iglast"):
        arrived(ig_ref.at[pl.ds(0, half), :], ("whole", 0))

    with SC("ruwait"): arrived(ru_ref.at[:, pl.ds(0, (R - 1) * h)], "ru")

    with SC("sendwait"):
        sent(tok.at[:, pl.ds(0, (4 * R + 3) * pr + others * h // D), :], "late")
    for names, sems in ((send_names, send_sems), (recv_names, recv_sems)):
        assert sum(n for _, n in names.values()) == sems.shape[0], (names, sems.shape)


def in_planes(R, hidden_in, cotangent, w_up, w_down):
    tl, D = hidden_in.shape
    dl, fl = w_up.shape
    T, h, pr = tl * R, fl // R, tl // 8
    send_sems, recv_sems = 3, 7 * R + 2 + (3 * R + 1) * SUBS
    vmem = pl.BlockSpec(memory_space=pltpu.VMEM)
    input_grad, up, down = pl.pallas_call(
        functools.partial(kernel, R),
        out_shape=(
            pltpu.VMEM((tl, D), BF16),
            pltpu.VMEM((dl, fl), BF16),
            pltpu.VMEM((fl, dl), F32),
        ),
        in_specs=[pl.BlockSpec(memory_space=pl.ANY)] * 4,
        out_specs=(vmem, vmem, vmem),
        scratch_shapes=[
            pltpu.VMEM((fl, dl), BF16),
            pltpu.VMEM((2, pr, D), BF16),
            pltpu.VMEM((2, T, D), BF16),
            pltpu.VMEM((D, h), BF16),
            pltpu.VMEM((h, D), BF16),
            pltpu.VMEM((T, h), F32),
            pltpu.VMEM((T, h), BF16),
            pltpu.VMEM((h, T), BF16),
            pltpu.VMEM((h, T), BF16),
            pltpu.VMEM((T, D), BF16),
            pltpu.VMEM((R * 4 * pr, D), BF16),
            pltpu.VMEM((R, 2, SUBS, pr // SUBS, D), BF16),
            pltpu.VMEM((R, SUBS, pr // SUBS, D), BF16),
            pltpu.VMEM((R, 2, SUBS, pr // SUBS, D), BF16),
            pltpu.VMEM((D, h), BF16),
            pltpu.VMEM((h, D), BF16),
            pltpu.SemaphoreType.DMA((send_sems,)),
            pltpu.SemaphoreType.DMA((recv_sems,)),
            pltpu.SemaphoreType.DMA((5,)),
        ],
        compiler_params=pltpu.CompilerParams(
            collective_id=0, has_side_effects=True, vmem_limit_bytes=58 * 1024 * 1024
        ),
    )(hidden_in, cotangent, w_up, w_down)
    return written_out(input_grad, up, down)


def write_out(ig_ref, up_ref, down_ref, ig_out, up_out, down_out, wide, sems):
    whole = [
        pltpu.make_async_copy(down_ref, down_out, sems.at[0]),
        pltpu.make_async_copy(ig_ref, ig_out, sems.at[1]),
    ]
    for copy in whole:
        copy.start()
    n = up_ref.shape[0] // CHUNKS
    for i in range(CHUNKS):
        at = pl.ds(i * n, n)
        wide[at, :] = up_ref[at, :].astype(F32)
        pltpu.make_async_copy(wide.at[at, :], up_out.at[at, :], sems.at[2]).start()
    for copy in whole + [pltpu.make_async_copy(wide, up_out, sems.at[2])]:
        copy.wait()


def written_out(input_grad, up, down):
    vmem = pl.BlockSpec(memory_space=pltpu.VMEM)
    there = [pltpu.with_memory_space_constraint(x, pltpu.VMEM) for x in (input_grad, up, down)]
    return pl.pallas_call(
        write_out,
        out_shape=(
            jax.ShapeDtypeStruct(input_grad.shape, BF16),
            jax.ShapeDtypeStruct(up.shape, F32),
            jax.ShapeDtypeStruct(down.shape, F32),
        ),
        in_specs=[vmem] * 3,
        out_specs=[pl.BlockSpec(memory_space=pl.ANY)] * 3,
        scratch_shapes=[pltpu.VMEM(up.shape, F32), pltpu.SemaphoreType.DMA((3,))],
        compiler_params=pltpu.CompilerParams(vmem_limit_bytes=8 * 1024 * 1024),
    )(*there)


def solution(mesh):
    R, F, C = (mesh.shape[name] for name in ("rep", "fs", "tp"))
    body = functools.partial(in_planes, R) if (R, F, C) == (4, 4, 2) else plain
    return jax.shard_map(
        body,
        mesh=mesh,
        in_specs=(P("rep", None), P("rep", None), P("rep", ("fs", "tp")), P(("fs", "tp"), "rep")),
        out_specs=(P("rep", None), P("rep", ("fs", "tp")), P(("fs", "tp"), "rep")),
        check_vma=False,
    )
```
